32 devices in a mesh: rep: 2 (over core), fs: 8 (over z, y), tp: 2 (over x).
Axes of the slice: x: 2, y: 2, z: 4, core: 2. Of those that a mesh axis runs over, the one named last changes fastest.
Arguments:
- residual: bfloat16 [2048, 4096], P('tp', ('rep', 'fs')), may hold values from -6 to 6
- mixer_gain: float32 [2048], replicated, may hold values from 0.1 to 1.9
- value_weight: float32 [2048, 512], P('fs', 'tp'), may hold values from -0.125 to 0.125
- value_scale: float32 [512], P('tp'), may hold values from 0.2 to 8, as said below
- input_gate_weight: float32 [2048, 512], P('fs', 'tp'), may hold values from -0.125 to 0.125
- input_gate_scale: float32 [512], P('tp'), may hold values from 0.5 to 2
- output_gate_weight: float32 [2048, 512], P('fs', 'tp'), may hold values from -0.125 to 0.125
- output_gate_scale: float32 [512], P('tp'), may hold values from 0.5 to 2
- conv_taps: float32 [3, 512], P(None, 'tp'), may hold values from -3 to 3
- conv_gain: float32 [512], P('tp'), may hold values from 0.1 to 1.9
- mixer_out_weight: float32 [512, 2048], P('tp', 'fs'), may hold values from -0.25 to 0.25
- mixer_out_scale: float32 [2048], P('fs'), may hold values from 0.5 to 2
- channel_gain: float32 [2048], replicated, may hold values from 0.1 to 1.9
- gate_weight: float32 [2048, 5632], P('fs', 'tp'), may hold values from -0.125 to 0.125
- gate_scale: float32 [5632], P('tp'), may hold values from 0.5 to 2
- up_weight: float32 [2048, 5632], P('fs', 'tp'), may hold values from -0.125 to 0.125
- up_scale: float32 [5632], P('tp'), may hold values from 0.5 to 2
- down_weight: float32 [5632, 2048], P('tp', 'fs'), may hold values from -0.078125 to 0.078125
- down_scale: float32 [2048], P('fs'), may hold values from 0.5 to 2
Outputs:
- layer_out: bfloat16 [2048, 4096], P('tp', ('rep', 'fs'))
The draws below stay inside these ranges and needn't reach their ends.
Inputs may be any that keep to these rules, and one draw needn't show every extreme that they name: `value_scale`: positive column scales.
All inputs are finite; a program needn't handle non-finite values.
Results may differ from the reference program's by a relative error of at most 0.018.
Values may be sent and summed in bfloat16 or wider, within the bound.
A program may use at most 128 MiB of HBM per device.

```python
import math
import jax
import jax.numpy as jnp
from jax import lax

D = 2048
C = 512
FF = 5632
TAPS = 3
LEN = 128
TOKENS = 4096
N_TP = 2


def draw_value_scale(key, part):
    index = jnp.arange(C, dtype=jnp.float32)
    ramp = 4.0 ** (index / C)
    rough = jnp.exp(jax.random.uniform(key, (C,), jnp.float32, -0.7, 0.7))
    return (0.5 * ramp * rough).astype(jnp.float32)


def shard_levels(own_key, shape, split, smallest, top_value):
    loudness = 1.0
    for dim, shards_of in split:
        heights = jax.random.uniform(jax.random.fold_in(jax.random.fold_in(own_key, 6), dim), (shards_of,), jnp.float32, smallest / len(split), top_value / len(split))
        loudness = loudness * jnp.repeat(jnp.exp(heights), shape[dim] // shards_of).reshape((-1,) + (1,) * (len(shape) - 1 - dim))
    return loudness


def scatter_about(own_key, extent, scale, most, pieces=(), kind=jnp.bfloat16):
    factor_of = shard_levels(own_key, extent, pieces, -0.22, 0.18) if pieces else 1.0
    values = jax.random.normal(own_key, extent, jnp.float32) * scale * factor_of
    return jnp.minimum(jnp.maximum(values, -most), most).astype(kind)


def setup_inputs(seed: int = 0) -> dict:
    key_of = jax.random.split(jax.random.key(seed), 20)
    residual = scatter_about(key_of[0], (D, TOKENS), 1.0, 6.0, ((0, 2), (1, 16)))
    mixer_gain = jnp.clip(1.0 + 0.18 * jax.random.normal(key_of[1], (D,), jnp.float32), 0.1, 1.9)
    value_weight = scatter_about(key_of[2], (D, C), D ** -0.5, 0.125, ((0, 8), (1, 2)), jnp.float32)
    value_scale = draw_value_scale(jax.random.fold_in(key_of[19], 71), 0)
    input_gate_weight = scatter_about(key_of[4], (D, C), D ** -0.5, 0.125, ((0, 8), (1, 2)), jnp.float32)
    input_gate_scale = jnp.clip(jnp.exp(math.log(2.0) - 1.3862944 * jax.random.uniform(key_of[5], (C,), jnp.float32) ** shard_levels(key_of[5], (C,), ((0, 2),), -0.2, 0.2)), 0.5, 2.0)
    output_gate_weight = scatter_about(key_of[6], (D, C), D ** -0.5, 0.125, ((0, 8), (1, 2)), jnp.float32)
    output_gate_scale = jnp.clip(jnp.exp(math.log(2.0) - 1.3862944 * jax.random.uniform(key_of[7], (C,), jnp.float32) ** shard_levels(key_of[7], (C,), ((0, 2),), -0.2, 0.2)), 0.5, 2.0)
    conv_taps = scatter_about(key_of[8], (TAPS, C), 0.577, 3.0, ((1, 2),), jnp.float32)
    conv_gain = jnp.clip(1.0 + 0.18 * jax.random.normal(key_of[9], (C,), jnp.float32), 0.1, 1.9)
    mixer_out_weight = scatter_about(key_of[10], (C, D), C ** -0.5, 0.25, ((0, 2), (1, 8)), jnp.float32)
    mixer_out_scale = jnp.clip(jnp.exp(math.log(2.0) - 1.3862944 * jax.random.uniform(key_of[11], (D,), jnp.float32) ** shard_levels(key_of[11], (D,), ((0, 8),), -0.2, 0.2)), 0.5, 2.0)
    channel_gain = jnp.clip(1.0 + 0.18 * jax.random.normal(key_of[12], (D,), jnp.float32), 0.1, 1.9)
    gate_weight = scatter_about(key_of[13], (D, FF), D ** -0.5, 0.125, ((0, 8), (1, 2)), jnp.float32)
    gate_scale = jnp.clip(jnp.exp(math.log(2.0) - 1.3862944 * jax.random.uniform(key_of[14], (FF,), jnp.float32) ** shard_levels(key_of[14], (FF,), ((0, 2),), -0.2, 0.2)), 0.5, 2.0)
    up_weight = scatter_about(key_of[15], (D, FF), D ** -0.5, 0.125, ((0, 8), (1, 2)), jnp.float32)
    up_scale = jnp.clip(jnp.exp(math.log(2.0) - 1.3862944 * jax.random.uniform(key_of[16], (FF,), jnp.float32) ** shard_levels(key_of[16], (FF,), ((0, 2),), -0.2, 0.2)), 0.5, 2.0)
    down_weight = scatter_about(key_of[17], (FF, D), FF ** -0.5, 0.078125, ((0, 2), (1, 8)), jnp.float32)
    down_scale = jnp.clip(jnp.exp(math.log(2.0) - 1.3862944 * jax.random.uniform(key_of[18], (D,), jnp.float32) ** shard_levels(key_of[18], (D,), ((0, 8),), -0.2, 0.2)), 0.5, 2.0)
    return dict(residual=residual, mixer_gain=mixer_gain, value_weight=value_weight, value_scale=value_scale, input_gate_weight=input_gate_weight, input_gate_scale=input_gate_scale, output_gate_weight=output_gate_weight, output_gate_scale=output_gate_scale, conv_taps=conv_taps, conv_gain=conv_gain, mixer_out_weight=mixer_out_weight, mixer_out_scale=mixer_out_scale, channel_gain=channel_gain, gate_weight=gate_weight, gate_scale=gate_scale, up_weight=up_weight, up_scale=up_scale, down_weight=down_weight, down_scale=down_scale)


epsilon = 1e-06

def normalize(values, gain):
    floats = values.astype(jnp.float32)
    mean = lax.optimization_barrier(jnp.mean(floats * floats, axis=0, keepdims=True))
    return (floats * lax.rsqrt(mean + epsilon) * gain[:, None]).astype(jnp.bfloat16)

def project(weight, rows):
    return jnp.dot(weight.T, rows, preferred_element_type=jnp.float32)

def causal_conv(values, taps):
    total = values.shape[1]
    position = jnp.arange(total, dtype=jnp.int32) % LEN
    shifted_one = jnp.pad(values, ((0, 0), (1, 0)))[:, :total]
    shifted_two = jnp.pad(values, ((0, 0), (2, 0)))[:, :total]
    shifted_one = jnp.where(position[None, :] >= 1, shifted_one, 0.0)
    shifted_two = jnp.where(position[None, :] >= 2, shifted_two, 0.0)
    return taps[2][:, None] * values + taps[1][:, None] * shifted_one + taps[0][:, None] * shifted_two

def block_sum(weight, rows, scale):
    width = weight.shape[0] // N_TP
    total = jnp.zeros((weight.shape[1], rows.shape[1]), jnp.float32)
    for block_index in range(N_TP):
        lower = block_index * width
        part = project(weight[lower:lower + width], rows[lower:lower + width]) * scale[:, None]
        rounded = lax.optimization_barrier(part.astype(jnp.bfloat16))
        total = total + rounded.astype(jnp.float32)
    return total

def reference(residual, mixer_gain, value_weight, value_scale, input_gate_weight, input_gate_scale, output_gate_weight, output_gate_scale, conv_taps, conv_gain, mixer_out_weight, mixer_out_scale, channel_gain, gate_weight, gate_scale, up_weight, up_scale, down_weight, down_scale):
    normed = normalize(residual, mixer_gain)
    value = project(value_weight.astype(jnp.bfloat16), normed) * value_scale[:, None]
    in_gate = project(input_gate_weight.astype(jnp.bfloat16), normed) * input_gate_scale[:, None]
    out_gate = project(output_gate_weight.astype(jnp.bfloat16), normed) * output_gate_scale[:, None]
    mixed = out_gate * causal_conv(in_gate * value, conv_taps)
    mean = lax.optimization_barrier(jnp.mean(mixed * mixed, axis=0, keepdims=True))
    conv_normed = (mixed * lax.rsqrt(mean + epsilon) * conv_gain[:, None]).astype(jnp.bfloat16)
    total = block_sum(mixer_out_weight.astype(jnp.bfloat16), conv_normed, mixer_out_scale)
    after_mixer = (residual.astype(jnp.float32) + total).astype(jnp.bfloat16)
    normed_two = normalize(after_mixer, channel_gain)
    gate = project(gate_weight.astype(jnp.bfloat16), normed_two) * gate_scale[:, None]
    upper = project(up_weight.astype(jnp.bfloat16), normed_two) * up_scale[:, None]
    hidden = (jax.nn.silu(gate) * upper).astype(jnp.bfloat16)
    total_two = block_sum(down_weight.astype(jnp.bfloat16), hidden, down_scale)
    return (after_mixer.astype(jnp.float32) + total_two).astype(jnp.bfloat16)
```

```python
import functools

import jax
import jax.numpy as jnp
from jax import lax
from jax.experimental import pallas as pl
from jax.experimental.pallas import tpu as pltpu
from jax.sharding import PartitionSpec as P

LEN = 128
MESH = pl.DeviceIdType.MESH

epsilon = 1e-06


def contract(weight, rows):
    return lax.dot_general(
        weight, rows, (((0,), (0,)), ((), ())), preferred_element_type=jnp.float32
    )


def normalize(values, gain):
    floats = values.astype(jnp.float32)
    mean = jnp.mean(floats * floats, axis=0, keepdims=True)
    return (floats * lax.rsqrt(mean + epsilon) * gain[:, None]).astype(jnp.bfloat16)


def causal_conv(values, taps, length):
    total = values.shape[1]
    position = jnp.arange(total, dtype=jnp.int32) % length
    shifted_one = jnp.pad(values, ((0, 0), (1, 0)))[:, :total]
    shifted_two = jnp.pad(values, ((0, 0), (2, 0)))[:, :total]
    shifted_one = jnp.where(position[None, :] >= 1, shifted_one, 0.0)
    shifted_two = jnp.where(position[None, :] >= 2, shifted_two, 0.0)
    return (
        taps[2][:, None] * values + taps[1][:, None] * shifted_one + taps[0][:, None] * shifted_two
    )


def ring_plan(sizes, ring):
    free = {"up": 0.0, "down": 0.0, "y": 0.0, "d": 0.0}
    rate = {"up": 46.0, "down": 46.0, "y": 46.0, "d": 330.0}
    waiting = []
    for array in range(len(sizes)):
        for chunk in range(4):
            waiting.append((0.0, array, chunk, 0, 0, None))
    order = []
    pending = []

    def push(ready, send, link, needs):
        pending.append((ready, send, link, needs))

    def ahead(ready, array, chunk, pair, hop, needs):
        link = "up" if chunk % 2 == 0 else "down"
        if hop < ring - 1:
            push(ready, (array, chunk, pair, hop, "z"), link, needs)
        if chunk < 2 and pair == 0 and hop == 0:
            push(ready, (array, chunk, pair, hop, "y"), "y", needs)
        if chunk >= 2 and pair == 0:
            push(ready, (array, chunk, pair, hop, "y"), "y", needs)
        if needs is not None:
            push(ready, (array, chunk, pair, hop, "d"), "d", needs)

    for _, array, chunk, pair, hop, needs in waiting:
        ahead(0.0, array, chunk, pair, hop, needs)
    while pending:
        best = min(
            range(len(pending)),
            key=lambda i: (
                max(pending[i][0], free[pending[i][2]]),
                pending[i][1][0],
                pending[i][0],
                i,
            ),
        )
        ready, send, link, needs = pending.pop(best)
        begin = max(ready, free[link])
        end = begin + sizes[send[0]] / rate[link] / 1e3
        free[link] = end
        order.append((begin, ready, send, needs))
        array, chunk, pair, hop, kind = send
        if kind == "z":
            ahead(end + 2.0, array, chunk, pair, hop + 1, send)
        elif kind == "y":
            if chunk < 2:
                ahead(end + 2.0, array, chunk, 1, 0, send)
            else:
                push(end + 2.0, (array, chunk, 1, hop, "d"), "d", send)
    order.sort(key=lambda item: item[1])
    return [(send, needs) for _, _, send, needs in order]


def gather_kernel(plan, count, groups, shards, *refs):
    own, (own_rows, own_scales) = refs[:count], refs[count : count + 2]
    outs = refs[count + 2 : 2 * count + 2]
    out_rows, out_scales = refs[2 * count + 2 : 2 * count + 4]
    send_sem, recv_sem, local_sem, small_send, small_recv = refs[2 * count + 4 :]
    ring = shards // 2
    place = lax.axis_index("fs")
    core = lax.axis_index("rep")
    group = lax.axis_index("tp")
    z, y = place // 2, place % 2
    up = {"fs": lax.rem(z + 1, ring) * 2 + y}
    down = {"fs": lax.rem(z + ring - 1, ring) * 2 + y}
    across = {"fs": z * 2 + (1 - y)}
    twin = {"rep": 1 - core}

    barrier = pltpu.get_barrier_semaphore()
    others = [{"fs": lax.rem(place + step, shards)} for step in range(1, shards)]
    others += [{"tp": lax.rem(group + step, groups)} for step in range(1, groups)]
    others += [twin]
    for other in others:
        pl.semaphore_signal(barrier, inc=1, device_id=other, device_id_type=MESH)
    pl.semaphore_wait(barrier, len(others))

    small = []
    for step in range(1, groups):
        small.append(
            pltpu.make_async_remote_copy(
                own_rows, out_rows.at[group], small_send.at[step - 1], small_recv.at[step - 1],
                device_id={"tp": lax.rem(group + step, groups)}, device_id_type=MESH,
            )
        )
    for step in range(1, shards):
        index = groups - 1 + step - 1
        small.append(
            pltpu.make_async_remote_copy(
                own_scales, out_scales.at[place], small_send.at[index], small_recv.at[index],
                device_id={"fs": lax.rem(place + step, shards)}, device_id_type=MESH,
            )
        )
    for copy in small:
        copy.start()

    copies = {}
    for number, (send, _) in enumerate(plan):
        array, chunk, pair, hop, kind = send
        step = hop if chunk % 2 == 0 else ring - hop
        owner = lax.rem(z + ring - step, ring) * 2 + (y if pair == 0 else 1 - y)
        slot = outs[array].at[owner, core, chunk]
        source = own[array].at[core, chunk] if (hop == 0 and pair == 0) else slot
        target = {"z": up if chunk % 2 == 0 else down, "y": across, "d": twin}[kind]
        copies[send] = pltpu.make_async_remote_copy(
            source, slot, send_sem.at[number], recv_sem.at[number],
            device_id=target, device_id_type=MESH,
        )

    local = [
        pltpu.make_async_copy(own[array], outs[array].at[place], local_sem.at[array])
        for array in range(count)
    ]
    local.append(pltpu.make_async_copy(own_rows, out_rows.at[group], local_sem.at[count]))
    local.append(pltpu.make_async_copy(own_scales, out_scales.at[place], local_sem.at[count + 1]))

    arrived = set()
    started_local = False
    for send, needs in plan:
        if needs is not None and needs not in arrived:
            if not started_local:
                started_local = True
                for copy in local:
                    copy.start()
            copies[needs].wait_recv()
            arrived.add(needs)
        copies[send].start()
    for send, _ in plan:
        copies[send].wait_send()
        if send not in arrived:
            copies[send].wait_recv()
    for copy in small:
        copy.wait()
    for copy in local:
        copy.wait()


def gather_all(arrays, rows, scales, groups, shards, reps):
    count = len(arrays)
    own = [a.reshape(reps, 4, a.shape[0] // (4 * reps), a.shape[1]) for a in arrays]
    sizes = [a.size // (4 * reps) * a.dtype.itemsize for a in arrays]
    plan = ring_plan(sizes, shards // 2)
    small = groups - 1 + shards - 1
    result = pl.pallas_call(
        functools.partial(gather_kernel, plan, count, groups, shards),
        out_shape=[jax.ShapeDtypeStruct((shards,) + a.shape, a.dtype) for a in own]
        + [
            jax.ShapeDtypeStruct((groups,) + rows.shape, rows.dtype),
            jax.ShapeDtypeStruct((shards,) + scales.shape, scales.dtype),
        ],
        in_specs=[pl.BlockSpec(memory_space=pl.ANY)] * (count + 2),
        out_specs=[pl.BlockSpec(memory_space=pl.ANY)] * (count + 2),
        scratch_shapes=[
            pltpu.SemaphoreType.DMA((len(plan),)),
            pltpu.SemaphoreType.DMA((len(plan),)),
            pltpu.SemaphoreType.DMA((count + 2,)),
            pltpu.SemaphoreType.DMA((small,)),
            pltpu.SemaphoreType.DMA((small,)),
        ],
        compiler_params=pltpu.CompilerParams(collective_id=0, has_side_effects=True),
        name="gather_all",
    )(*own, rows, scales)
    whole = [g.reshape((shards,) + a.shape) for g, a in zip(result, arrays)]
    return whole, result[count], result[count + 1]


def layer_kernel(
    channels, length,
    own_res, mixer_gain, mix_scales, taps, own_gain, channel_gain, gate_scale, up_scale, own_scales,
    *refs,
):
    raw, out_ref, refs = refs[:7], refs[7], refs[8:]
    bufs, refs = refs[:5], refs[5:]
    others, refs = refs[:5], refs[5:]
    stages, refs = refs[:7], refs[7:]
    (res, scales, gains, mixes, after, normed, gate_buf, hidden, outgoing, from_x, to_z, from_z,
     raw_sem, z_send, z_recv, y_send, y_recv, t_send, t_recv, mx_send, mx_recv, mt_send, mt_recv,
     r_send, r_recv, s_send, s_recv, m_send, m_recv, px_send, px_recv, pz_send, pz_recv) = refs
    proj_buf, mout_buf, gate_w, up_w, down_w = bufs
    shards = gate_w.shape[0]
    place = lax.axis_index("fs")
    core = lax.axis_index("rep")
    group = lax.axis_index("tp")
    tokens, own_width = own_res.shape
    features = 2 * own_width
    block = mout_buf.shape[-1]
    per_group = shards // 2
    depth = shards // 2
    width = gate_w.shape[-1]
    narrow = mixes.shape[-1]
    all_tokens = 2 * tokens

    z, y = place // 2, place % 2
    side = z % 2
    part_of = ((z + 1) // 2) % 2
    high = (z * 2 + y) // per_group
    pair = z + 1 - 2 * side
    inner = part_of == 1
    outer = part_of == 0
    opposite = 1 - z // 2
    levels = [z, pair, 1 + opposite, (depth - 1) * opposite]
    twin = {"rep": 1 - core}
    across = {"fs": z * 2 + 1 - y}
    beside = {"tp": 1 - group}
    mate = {"fs": pair * 2 + y}
    corner = {"fs": pair * 2 + y, "tp": 1 - group}

    def remote(source, target, send, recv, device):
        return pltpu.make_async_remote_copy(
            source, target, send, recv, device_id=device, device_id_type=MESH
        )

    def spot(array, owner, half):
        if array == 1:
            return mout_buf.at[owner, group, half]
        if array >= 4:
            return down_w.at[owner, half, array - 4]
        return bufs[array].at[owner, half]

    def owner_of(r, far):
        return levels[r] * 2 + (1 - y if far else y)

    def z_copy(array, way):
        target = spot(array, place, core)
        if array == 1 or way == 2:
            source = target
        else:
            source = others[array - 1 if array else 0]
        level = (None, pair, depth - 1 - z, depth - 1 - pair)[way]
        kind = 0 if way == 1 else 2 - part_of
        return remote(
            source, target, z_send.at[array, way - 1], z_recv.at[array, kind],
            {"fs": level * 2 + y},
        )

    def z_wait(array, r):
        target = spot(array, owner_of(r, False), core)
        remote(
            target, target, z_send.at[array, r - 1], z_recv.at[array, r - 1], across
        ).wait_recv()

    def y_copy(array, r):
        target = spot(array, owner_of(r, False), core)
        return remote(target, target, y_send.at[array, r], y_recv.at[array, r], across)

    def t_copy(array, r, far):
        target = spot(array, owner_of(r, far), core)
        index = r + 4 * far
        return remote(target, target, t_send.at[array, index], t_recv.at[array, index], twin)

    def mx_copy(r, far):
        target = spot(1, owner_of(r, far), core)
        index = r + 4 * far
        return remote(target, target, mx_send.at[index], mx_recv.at[index], beside)

    def mt_copy(r, far):
        target = mout_buf.at[owner_of(r, far), 1 - group, core]
        index = r + 4 * far
        return remote(target, target, mt_send.at[index], mt_recv.at[index], twin)

    rows = stages[0].shape[0]
    tall = stages[6].shape[1]
    raw_copies = []
    for i in range(4):
        raw_copies.append([pltpu.make_async_copy(
            raw[i].at[pl.ds(pl.multiple_of(core * rows, rows), rows)], stages[i], raw_sem.at[i])])
    for i in range(4, 6):
        raw_copies.append([pltpu.make_async_copy(
            raw[i].at[pl.ds(pl.multiple_of(core * rows, rows), rows)], stages[i], raw_sem.at[i])])
    raw_copies.append([
        pltpu.make_async_copy(
            raw[6].at[pl.ds(pl.multiple_of(k * width + core * tall, 16), tall)],
            stages[6].at[k], raw_sem.at[6 + k])
        for k in range(2)
    ])
    for group_of in raw_copies:
        for copy in group_of:
            copy.start()

    barrier = pltpu.get_barrier_semaphore()
    partners = [{"fs": lax.rem(place + step, shards)} for step in range(1, shards)]
    partners += [beside, corner, twin]
    for other in partners:
        pl.semaphore_signal(barrier, inc=1, device_id=other, device_id_type=MESH)
    pl.semaphore_wait(barrier, len(partners))

    scale_copies = [
        remote(own_scales, scales.at[place], s_send.at[step], s_recv.at[step],
               {"fs": lax.rem(place + step, shards)})
        for step in range(1, shards)
    ]
    scale_copies.append(remote(own_gain, gains.at[group], s_send.at[0], s_recv.at[0], beside))
    res_z = remote(own_res, res.at[side, group], r_send.at[0], r_recv.at[0], mate)
    res_x = remote(own_res, res.at[side, group], r_send.at[1], r_recv.at[1], beside)
    passed = res.at[1 - side, group]
    res_d = remote(passed, passed, r_send.at[2], r_recv.at[2], beside)

    def start_z(*pairs):
        for array, r in pairs:
            z_copy(array, r).start()

    def wait_raw(*indices):
        for i in indices:
            for copy in raw_copies[i]:
                copy.wait()

    def both(first, second, size):
        return [
            (first, pl.ds(pl.multiple_of(part_of * size, 128), size)),
            (second, pl.ds(pl.multiple_of((1 - part_of) * size, 128), size)),
        ]

    res_z.start()
    res_x.start()
    wait_raw(0, 1, 2)
    for i in range(3):
        for target, cols in both(proj_buf.at[place, core], others[0], narrow):
            target[:, i * narrow : (i + 1) * narrow] = stages[i][:, cols].astype(jnp.bfloat16)
    start_z((0, 1), (0, 2), (0, 3))
    y_copy(0, 0).start()
    t_copy(0, 0, False).start()
    wait_raw(3)
    mout_buf[place, group, core] = stages[3][...].astype(jnp.bfloat16)
    start_z((1, 1), (1, 2), (1, 3))
    y_copy(1, 0).start()
    mx_copy(0, False).start()
    t_copy(1, 0, False).start()
    for copy in scale_copies:
        copy.start()
    for array in (2, 3):
        wait_raw(array + 2)
        for target, cols in both(bufs[array].at[place, core], others[array - 1], width):
            target[...] = stages[array + 2][:, cols].astype(jnp.bfloat16)
        t_copy(array, 0, False).start()
        if array == 2:
            y_copy(2, 0).start()
            start_z((2, 1))

        @pl.when(inner)
        def _():
            start_z((array, 2), (array, 3))
    wait_raw(6)
    short = tall // 2
    for k, array in ((0, 4), (1, 5)):
        lines = slice(k * short, (k + 1) * short)
        down_w[place, core, k] = stages[6][part_of, lines, :].astype(jnp.bfloat16)
        others[array - 1][...] = stages[6][1 - part_of, lines, :].astype(jnp.bfloat16)
    for array in (4, 5):
        t_copy(array, 0, False).start()
    res[side, group] = own_res[...]
    scales[place] = own_scales[...]
    gains[group] = own_gain[...]

    def take_z(array, r):
        z_wait(array, r)
        y_copy(array, r).start()
        t_copy(array, r, False).start()
        if array == 1:
            mx_copy(r, False).start()

    def take_y(array, r):
        y_copy(array, r).wait_recv()
        t_copy(array, r, True).start()
        if array == 1:
            mx_copy(r, True).start()

    def finish(array):
        for far in (False, True):
            for r in range(4):
                t_copy(array, r, far).wait_recv()

    def scaled(squares, count):
        return lax.rsqrt(squares / count + epsilon)

    def normalize_side(s):
        floats = [res[s, k].astype(jnp.float32) for k in range(2)]
        squares = sum(jnp.sum(row * row, axis=1, keepdims=True) for row in floats)
        factor = scaled(squares, features)
        lines = pl.ds(pl.multiple_of(s * tokens, tokens), tokens)
        for k in range(2):
            cols = slice(k * own_width, (k + 1) * own_width)
            normed[lines, cols] = (
                res[s, k].astype(jnp.float32) * factor * mixer_gain[:, cols]
            ).astype(jnp.bfloat16)

    order = (1, 2, 3)
    take_z(0, 2)
    take_z(1, 2)
    res_z.wait_recv()
    res_d.start()
    for r in (1, 3):
        take_z(0, r)
    for r in (1, 3):
        take_z(1, r)
    y_copy(3, 0).start()
    take_z(2, 2)
    res_x.wait_recv()
    normalize_side(side)
    for r in (0,) + order:
        take_y(0, r)
    for r in (0,) + order:
        take_y(1, r)
    res_d.wait_recv()
    normalize_side(1 - side)
    finish(0)

    own_cols = pl.ds(pl.multiple_of(part_of * narrow, 128), narrow)

    def project(index):
        weight = proj_buf[:, :, :, index * narrow : (index + 1) * narrow].reshape(features, narrow)
        product = jnp.dot(normed[...], weight, preferred_element_type=jnp.float32)
        return product * mix_scales[index : index + 1, own_cols]

    value = project(0)
    u = project(1) * value
    place_in = lax.rem(lax.broadcasted_iota(jnp.int32, u.shape, 0), length)
    one = jnp.where(place_in >= 1, pltpu.roll(u, 1, 0), 0.0)
    two = jnp.where(place_in >= 2, pltpu.roll(u, 2, 0), 0.0)
    conv = taps[2:3, own_cols] * u + taps[1:2, own_cols] * one + taps[0:1, own_cols] * two
    mixes[group, part_of] = (project(2) * conv).astype(jnp.bfloat16)
    mix_slot = mixes.at[group, part_of]
    mix_copies = [
        remote(mix_slot, mix_slot, m_send.at[i], m_recv.at[i], device)
        for i, device in enumerate((mate, beside, corner))
    ]
    for copy in mix_copies:
        copy.start()
    start_z((3, 1))

    @pl.when(outer)
    def _():
        start_z((2, 2), (2, 3))

    start_z((4, 1), (5, 1))

    @pl.when(outer)
    def _():
        start_z((3, 2), (3, 3))

    take_z(2, 1)
    for array in (4, 5):
        y_copy(array, 0).start()
    for far in (False, True):
        for r in range(4):
            mx_copy(r, far).wait_recv()
            mt_copy(r, far).start()
    for copy in scale_copies + mix_copies:
        copy.wait_recv()
    finish(1)
    for far in (False, True):
        for r in range(4):
            mt_copy(r, far).wait_recv()
    total = jnp.zeros((all_tokens, 1), jnp.float32)
    for k in range(2):
        for b in range(2):
            lines = mixes[k, b].astype(jnp.float32)
            total = total + jnp.sum(lines * lines, axis=1, keepdims=True)
    factor = scaled(total, channels)
    for k in range(2):
        for b in range(2):
            cols = slice((2 * k + b) * narrow, (2 * k + b + 1) * narrow)
            hidden[:, cols] = (
                mixes[k, b].astype(jnp.float32) * factor
                * gains[k, 0:1, b * narrow : (b + 1) * narrow]
            ).astype(jnp.bfloat16)
    squares = jnp.zeros((all_tokens, 1), jnp.float32)
    for s in range(shards):
        k, inside = s // per_group, (s % per_group) * block
        part = jnp.dot(
            hidden[:, : 4 * narrow], mout_buf[s].reshape(4 * narrow, block),
            preferred_element_type=jnp.float32,
        ) * scales[s, 0:1, :]
        base = res[:, k, :, inside : inside + block].reshape(all_tokens, block)
        row = (base.astype(jnp.float32) + part).astype(jnp.bfloat16)
        after[s] = row
        row = row.astype(jnp.float32)
        squares = squares + jnp.sum(row * row, axis=1, keepdims=True)
    factor = scaled(squares, features)
    for s in range(shards):
        cols = slice(s * block, (s + 1) * block)
        normed[:, cols] = (
            after[s].astype(jnp.float32) * factor * channel_gain[:, cols]
        ).astype(jnp.bfloat16)

    def tiles(body):
        tile = 256
        whole = width // tile

        @pl.loop(0, whole)
        def _(j):
            body(pl.multiple_of(j * tile, tile), tile)

        if width % tile:
            body(whole * tile, width % tile)

    def multiply(weights, start, size):
        weight = weights[:, :, :, pl.ds(start, size)].reshape(features, size)
        return jnp.dot(normed[...], weight, preferred_element_type=jnp.float32)

    def scale_at(scale, start, size):
        return scale[:, pl.ds(pl.multiple_of(part_of * width + start, 128), size)]

    def gate_tile(start, size):
        gate_buf[:, pl.ds(start, size)] = multiply(gate_w, start, size) * scale_at(
            gate_scale, start, size
        )

    def up_tile(start, size):
        product = multiply(up_w, start, size) * scale_at(up_scale, start, size)
        gate = gate_buf[:, pl.ds(start, size)]
        hidden[:, pl.ds(start, size)] = (
            gate / (1.0 + jnp.exp(-gate)) * product
        ).astype(jnp.bfloat16)

    take_z(3, 2)
    take_z(3, 1)
    take_z(2, 3)
    for r in (0,) + order:
        take_y(2, r)
    finish(2)
    tiles(gate_tile)
    take_z(4, 1)
    take_z(5, 1)
    take_z(3, 3)
    start_z((4, 2), (4, 3), (5, 2), (5, 3))
    for r in (0,) + order:
        take_y(3, r)
    finish(3)
    tiles(up_tile)

    steps = [(r, far) for r in range(4) for far in (False, True)]

    def index_of(k):
        return owner_of(*steps[k])

    def mine(k):
        return (high == group) if k < per_group else (high != group)

    def slot_of(k):
        return lax.rem(index_of(k), per_group)

    def px_copy(k, which):
        who = 1 - side if which == 0 else side
        return remote(
            outgoing.at[k, who], from_x.at[k, who], px_send.at[k, which], px_recv.at[k, which], beside
        )

    def pz_copy(k):
        i = slot_of(k)
        return remote(to_z.at[i], from_z.at[i], pz_send.at[i], pz_recv.at[i], mate)

    def down(k):
        r, far = steps[k]
        for array in (4, 5):
            t_copy(array, r, far).wait_recv()
        s = index_of(k)
        weight = down_w[s].reshape(width, block)
        part = jnp.dot(hidden[...], weight, preferred_element_type=jnp.float32)
        part = (part * scales[s, 1:2, :]).astype(jnp.bfloat16)
        outgoing[k, 0] = part[:tokens]
        outgoing[k, 1] = part[tokens:]

        @pl.when(jnp.logical_not(mine(k)))
        def _():
            px_copy(k, 0).start()
            px_copy(k, 1).start()

    def pass_on(k):
        @pl.when(mine(k))
        def _():
            px_copy(k, 0).wait_recv()
            to_z[slot_of(k)] = (
                outgoing[k, 1 - side].astype(jnp.float32) + from_x[k, 1 - side].astype(jnp.float32)
            ).astype(jnp.bfloat16)
            pz_copy(k).start()

    def close(k):
        i = slot_of(k)
        s = index_of(k)

        @pl.when(mine(k))
        def _():
            px_copy(k, 1).wait_recv()
            pz_copy(k).wait_recv()
            lines = pl.ds(pl.multiple_of(side * tokens, tokens), tokens)
            total = outgoing[k, side].astype(jnp.float32) + from_x[k, side].astype(jnp.float32)
            total = total + from_z[i].astype(jnp.float32)
            out_ref[:, pl.ds(pl.multiple_of(i * block, block), block)] = (
                after[s, lines, :].astype(jnp.float32) + total
            ).astype(jnp.bfloat16)

    def take_all(take, r):
        for array in (4, 5):
            take(array, r)

    down(0)
    take_all(take_y, 0)
    down(1)
    down(2)
    take_all(take_y, 1)
    down(3)
    take_all(take_z, 2)
    down(4)
    pass_on(0)
    pass_on(1)
    take_all(take_y, 2)
    down(5)
    pass_on(2)
    pass_on(3)
    take_all(take_z, 3)
    pass_on(4)
    down(6)
    pass_on(5)
    take_all(take_y, 3)
    down(7)
    for k in range(per_group):
        close(k)
    pass_on(6)
    pass_on(7)
    for k in range(per_group, shards):
        close(k)

    for array in range(6):
        for r in range(4):
            if r:
                z_copy(array, r).wait_send()
            y_copy(array, r).wait_send()
            for far in (False, True):
                t_copy(array, r, far).wait_send()
    for r in range(4):
        for far in (False, True):
            mx_copy(r, far).wait_send()
            mt_copy(r, far).wait_send()
    for copy in scale_copies + mix_copies + [res_z, res_x, res_d]:
        copy.wait_send()
    for k in range(len(steps)):
        @pl.when(mine(k))
        def _():
            pz_copy(k).wait_send()

        @pl.when(jnp.logical_not(mine(k)))
        def _():
            px_copy(k, 0).wait_send()
            px_copy(k, 1).wait_send()


def fused(
    shards, residual, mixer_gain, mix_scales, taps, conv_gain, channel_gain,
    gate_scale, up_scale, scales, raw,
):
    tokens, own_width = residual.shape
    features = 2 * own_width
    short = jnp.bfloat16
    in_rows, mix_width = raw[0].shape
    rows, narrow = in_rows // 2, mix_width // 2
    ff = gate_scale.shape[1]
    width = ff // 2
    out_rows, block = raw[3].shape
    channels = 2 * out_rows
    tall = width // 2
    steps = shards
    vmem = pl.BlockSpec(memory_space=pltpu.VMEM)
    dma = pltpu.SemaphoreType.DMA
    return pl.pallas_call(
        functools.partial(layer_kernel, channels, LEN),
        out_shape=jax.ShapeDtypeStruct((tokens, own_width), short),
        in_specs=[vmem] * 9 + [pl.BlockSpec(memory_space=pl.ANY)] * 7,
        out_specs=vmem,
        scratch_shapes=[
            pltpu.VMEM((shards, 2, rows, 3 * narrow), short),
            pltpu.VMEM((shards, 2, 2, out_rows // 2, block), short),
            pltpu.VMEM((shards, 2, rows, width), short),
            pltpu.VMEM((shards, 2, rows, width), short),
            pltpu.VMEM((shards, 2, 2, tall // 2, block), short),
            pltpu.VMEM((rows, 3 * narrow), short),
            pltpu.VMEM((rows, width), short),
            pltpu.VMEM((rows, width), short),
            pltpu.VMEM((tall // 2, block), short),
            pltpu.VMEM((tall // 2, block), short),
        ]
        + [pltpu.VMEM((rows, mix_width), jnp.float32)] * 3
        + [
            pltpu.VMEM((out_rows // 2, block), jnp.float32),
            pltpu.VMEM((rows, ff), jnp.float32),
            pltpu.VMEM((rows, ff), jnp.float32),
            pltpu.VMEM((2, tall, block), jnp.float32),
            pltpu.VMEM((2, 2, tokens, own_width), short),
            pltpu.VMEM((shards,) + scales.shape, jnp.float32),
            pltpu.VMEM((2,) + conv_gain.shape, jnp.float32),
            pltpu.VMEM((2, 2, 2 * tokens, narrow), short),
            pltpu.VMEM((shards, 2 * tokens, block), short),
            pltpu.VMEM((2 * tokens, features), short),
            pltpu.VMEM((2 * tokens, width), jnp.float32),
            pltpu.VMEM((2 * tokens, width), short),
            pltpu.VMEM((steps, 2, tokens, block), short),
            pltpu.VMEM((steps, 2, tokens, block), short),
            pltpu.VMEM((steps // 2, tokens, block), short),
            pltpu.VMEM((steps // 2, tokens, block), short),
            dma((8,)),
            dma((6, 3)),
            dma((6, 3)),
            dma((6, 4)),
            dma((6, 4)),
            dma((6, 8)),
            dma((6, 8)),
            dma((8,)),
            dma((8,)),
            dma((8,)),
            dma((8,)),
            dma((3,)),
            dma((3,)),
            dma((shards,)),
            dma((shards,)),
            dma((3,)),
            dma((3,)),
            dma((steps, 2)),
            dma((steps, 2)),
            dma((steps // 2,)),
            dma((steps // 2,)),
        ],
        compiler_params=pltpu.CompilerParams(
            collective_id=1, has_side_effects=True, vmem_limit_bytes=60 * 1024 * 1024
        ),
        name="layer",
    )(
        residual, mixer_gain, mix_scales, taps, conv_gain, channel_gain, gate_scale, up_scale,
        scales, *raw,
    )


def local(
    reps,
    shards,
    groups,
    residual,
    mixer_gain,
    value_weight,
    value_scale,
    input_gate_weight,
    input_gate_scale,
    output_gate_weight,
    output_gate_scale,
    conv_taps,
    conv_gain,
    mixer_out_weight,
    mixer_out_scale,
    channel_gain,
    gate_weight,
    gate_scale,
    up_weight,
    up_scale,
    down_weight,
    down_scale,
):
    own_rows, tokens = residual.shape
    width = value_weight.shape[1]
    channels = width * groups
    features = own_rows * groups
    short = jnp.bfloat16
    block, ff = mixer_out_weight.shape[1], gate_weight.shape[1]
    in_rows, out_rows = value_weight.shape[0], mixer_out_weight.shape[0]
    if (
        reps == 2 and groups == 2 and shards == 8 and tokens % LEN == 0
        and block % 128 == 0 and width % 256 == 0 and ff % 256 == 0 and ff % 128 == 0
        and in_rows % 32 == 0 and out_rows == width and own_rows == block * shards // 2
    ):
        pad = jnp.zeros((7, width), jnp.float32)
        result = fused(
            shards, residual.T, mixer_gain[None],
            jnp.stack([value_scale, input_gate_scale, output_gate_scale]), conv_taps,
            jnp.concatenate([conv_gain[None], pad]), channel_gain[None], gate_scale[None], up_scale[None],
            jnp.pad(jnp.stack([mixer_out_scale, down_scale]), ((0, 6), (0, 0))),
            [value_weight, input_gate_weight, output_gate_weight, mixer_out_weight,
             gate_weight, up_weight, down_weight],
        )
        return result.T
    projections = jnp.concatenate(
        [value_weight.astype(short), input_gate_weight.astype(short), output_gate_weight.astype(short)],
        axis=1,
    )
    arrays = [
        projections,
        mixer_out_weight.astype(short),
        gate_weight.astype(short),
        up_weight.astype(short),
        down_weight.astype(short),
    ]
    scales = jnp.stack([mixer_out_scale, down_scale])
    (proj_all, out_all, gate_all, up_all, down_all), rows_all, scales_all = gather_all(
        arrays, residual, scales, groups, shards, reps
    )
    whole = rows_all.reshape(features, tokens)
    out_scale = scales_all[:, 0].reshape(features)
    down_scale_full = scales_all[:, 1].reshape(features)

    normed = normalize(whole, mixer_gain)
    projected = contract(proj_all.reshape(features, 3 * width), normed)
    value = projected[:width] * value_scale[:, None]
    in_gate = projected[width : 2 * width] * input_gate_scale[:, None]
    out_gate = projected[2 * width :] * output_gate_scale[:, None]
    mixed = out_gate * causal_conv(in_gate * value, conv_taps, LEN)
    squares = lax.psum(jnp.sum(mixed * mixed, axis=0), "tp")
    conv_normed = (
        mixed * lax.rsqrt(squares / channels + epsilon)[None, :] * conv_gain[:, None]
    ).astype(short)
    part = lax.dot_general(
        out_all, conv_normed, (((1,), (0,)), ((), ())), preferred_element_type=jnp.float32
    ).reshape(features, tokens)
    rounded = (part * out_scale[:, None]).astype(short)
    parts = lax.all_gather(rounded, "tp", axis=0)
    total = jnp.sum(parts.astype(jnp.float32), axis=0)
    after_whole = (whole.astype(jnp.float32) + total).astype(short)
    after_own = lax.dynamic_slice_in_dim(
        after_whole, lax.axis_index("tp") * own_rows, own_rows, 0
    )
    normed_two = normalize(after_whole, channel_gain)
    gate = contract(gate_all.reshape(features, -1), normed_two)
    upper = contract(up_all.reshape(features, -1), normed_two)
    hidden = (jax.nn.silu(gate * gate_scale[:, None]) * (upper * up_scale[:, None])).astype(short)
    down = lax.dot_general(
        down_all, hidden, (((1,), (0,)), ((), ())), preferred_element_type=jnp.float32
    ).reshape(features, tokens)
    total_two = lax.psum_scatter(
        (down * down_scale_full[:, None]).astype(short),
        "tp",
        scatter_dimension=0,
        tiled=True,
    ).astype(jnp.float32)
    return (after_own.astype(jnp.float32) + total_two).astype(short)


def solution(mesh):
    placed = (
        P("tp", ("rep", "fs")),
        P(),
        P("fs", "tp"),
        P("tp"),
        P("fs", "tp"),
        P("tp"),
        P("fs", "tp"),
        P("tp"),
        P(None, "tp"),
        P("tp"),
        P("tp", "fs"),
        P("fs"),
        P(),
        P("fs", "tp"),
        P("tp"),
        P("fs", "tp"),
        P("tp"),
        P("tp", "fs"),
        P("fs"),
    )
    sizes = mesh.shape["rep"], mesh.shape["fs"], mesh.shape["tp"]
    return jax.shard_map(
        functools.partial(local, *sizes),
        mesh=mesh,
        in_specs=placed,
        out_specs=P("tp", ("rep", "fs")),
        check_vma=False,
    )
```

```python
import functools

import jax
import jax.numpy as jnp
from jax import lax
from jax.experimental import pallas as pl
from jax.experimental.pallas import tpu as pltpu
from jax.sharding import PartitionSpec as P

LEN = 128
MESH = pl.DeviceIdType.MESH

epsilon = 1e-06


def contract(weight, rows):
    return lax.dot_general(
        weight, rows, (((0,), (0,)), ((), ())), preferred_element_type=jnp.float32
    )


def normalize(values, gain):
    floats = values.astype(jnp.float32)
    mean = jnp.mean(floats * floats, axis=0, keepdims=True)
    return (floats * lax.rsqrt(mean + epsilon) * gain[:, None]).astype(jnp.bfloat16)


def causal_conv(values, taps, length):
    total = values.shape[1]
    position = jnp.arange(total, dtype=jnp.int32) % length
    shifted_one = jnp.pad(values, ((0, 0), (1, 0)))[:, :total]
    shifted_two = jnp.pad(values, ((0, 0), (2, 0)))[:, :total]
    shifted_one = jnp.where(position[None, :] >= 1, shifted_one, 0.0)
    shifted_two = jnp.where(position[None, :] >= 2, shifted_two, 0.0)
    return (
        taps[2][:, None] * values + taps[1][:, None] * shifted_one + taps[0][:, None] * shifted_two
    )


def ring_plan(sizes, ring):
    free = {"up": 0.0, "down": 0.0, "y": 0.0, "d": 0.0}
    rate = {"up": 46.0, "down": 46.0, "y": 46.0, "d": 330.0}
    waiting = []
    for array in range(len(sizes)):
        for chunk in range(4):
            waiting.append((0.0, array, chunk, 0, 0, None))
    order = []
    pending = []

    def push(ready, send, link, needs):
        pending.append((ready, send, link, needs))

    def ahead(ready, array, chunk, pair, hop, needs):
        link = "up" if chunk % 2 == 0 else "down"
        if hop < ring - 1:
            push(ready, (array, chunk, pair, hop, "z"), link, needs)
        if chunk < 2 and pair == 0 and hop == 0:
            push(ready, (array, chunk, pair, hop, "y"), "y", needs)
        if chunk >= 2 and pair == 0:
            push(ready, (array, chunk, pair, hop, "y"), "y", needs)
        if needs is not None:
            push(ready, (array, chunk, pair, hop, "d"), "d", needs)

    for _, array, chunk, pair, hop, needs in waiting:
        ahead(0.0, array, chunk, pair, hop, needs)
    while pending:
        best = min(
            range(len(pending)),
            key=lambda i: (
                max(pending[i][0], free[pending[i][2]]),
                pending[i][1][0],
                pending[i][0],
                i,
            ),
        )
        ready, send, link, needs = pending.pop(best)
        begin = max(ready, free[link])
        end = begin + sizes[send[0]] / rate[link] / 1e3
        free[link] = end
        order.append((begin, ready, send, needs))
        array, chunk, pair, hop, kind = send
        if kind == "z":
            ahead(end + 2.0, array, chunk, pair, hop + 1, send)
        elif kind == "y":
            if chunk < 2:
                ahead(end + 2.0, array, chunk, 1, 0, send)
            else:
                push(end + 2.0, (array, chunk, 1, hop, "d"), "d", send)
    order.sort(key=lambda item: item[1])
    return [(send, needs) for _, _, send, needs in order]


def gather_kernel(plan, count, groups, shards, *refs):
    own, (own_rows, own_scales) = refs[:count], refs[count : count + 2]
    outs = refs[count + 2 : 2 * count + 2]
    out_rows, out_scales = refs[2 * count + 2 : 2 * count + 4]
    send_sem, recv_sem, local_sem, small_send, small_recv = refs[2 * count + 4 :]
    ring = shards // 2
    place = lax.axis_index("fs")
    core = lax.axis_index("rep")
    group = lax.axis_index("tp")
    z, y = place // 2, place % 2
    up = {"fs": lax.rem(z + 1, ring) * 2 + y}
    down = {"fs": lax.rem(z + ring - 1, ring) * 2 + y}
    across = {"fs": z * 2 + (1 - y)}
    twin = {"rep": 1 - core}

    barrier = pltpu.get_barrier_semaphore()
    others = [{"fs": lax.rem(place + step, shards)} for step in range(1, shards)]
    others += [{"tp": lax.rem(group + step, groups)} for step in range(1, groups)]
    others += [twin]
    for other in others:
        pl.semaphore_signal(barrier, inc=1, device_id=other, device_id_type=MESH)
    pl.semaphore_wait(barrier, len(others))

    small = []
    for step in range(1, groups):
        small.append(
            pltpu.make_async_remote_copy(
                own_rows, out_rows.at[group], small_send.at[step - 1], small_recv.at[step - 1],
                device_id={"tp": lax.rem(group + step, groups)}, device_id_type=MESH,
            )
        )
    for step in range(1, shards):
        index = groups - 1 + step - 1
        small.append(
            pltpu.make_async_remote_copy(
                own_scales, out_scales.at[place], small_send.at[index], small_recv.at[index],
                device_id={"fs": lax.rem(place + step, shards)}, device_id_type=MESH,
            )
        )
    for copy in small:
        copy.start()

    copies = {}
    for number, (send, _) in enumerate(plan):
        array, chunk, pair, hop, kind = send
        step = hop if chunk % 2 == 0 else ring - hop
        owner = lax.rem(z + ring - step, ring) * 2 + (y if pair == 0 else 1 - y)
        slot = outs[array].at[owner, core, chunk]
        source = own[array].at[core, chunk] if (hop == 0 and pair == 0) else slot
        target = {"z": up if chunk % 2 == 0 else down, "y": across, "d": twin}[kind]
        copies[send] = pltpu.make_async_remote_copy(
            source, slot, send_sem.at[number], recv_sem.at[number],
            device_id=target, device_id_type=MESH,
        )

    local = [
        pltpu.make_async_copy(own[array], outs[array].at[place], local_sem.at[array])
        for array in range(count)
    ]
    local.append(pltpu.make_async_copy(own_rows, out_rows.at[group], local_sem.at[count]))
    local.append(pltpu.make_async_copy(own_scales, out_scales.at[place], local_sem.at[count + 1]))

    arrived = set()
    started_local = False
    for send, needs in plan:
        if needs is not None and needs not in arrived:
            if not started_local:
                started_local = True
                for copy in local:
                    copy.start()
            copies[needs].wait_recv()
            arrived.add(needs)
        copies[send].start()
    for send, _ in plan:
        copies[send].wait_send()
        if send not in arrived:
            copies[send].wait_recv()
    for copy in small:
        copy.wait()
    for copy in local:
        copy.wait()


def gather_all(arrays, rows, scales, groups, shards, reps):
    count = len(arrays)
    own = [a.reshape(reps, 4, a.shape[0] // (4 * reps), a.shape[1]) for a in arrays]
    sizes = [a.size // (4 * reps) * a.dtype.itemsize for a in arrays]
    plan = ring_plan(sizes, shards // 2)
    small = groups - 1 + shards - 1
    result = pl.pallas_call(
        functools.partial(gather_kernel, plan, count, groups, shards),
        out_shape=[jax.ShapeDtypeStruct((shards,) + a.shape, a.dtype) for a in own]
        + [
            jax.ShapeDtypeStruct((groups,) + rows.shape, rows.dtype),
            jax.ShapeDtypeStruct((shards,) + scales.shape, scales.dtype),
        ],
        in_specs=[pl.BlockSpec(memory_space=pl.ANY)] * (count + 2),
        out_specs=[pl.BlockSpec(memory_space=pl.ANY)] * (count + 2),
        scratch_shapes=[
            pltpu.SemaphoreType.DMA((len(plan),)),
            pltpu.SemaphoreType.DMA((len(plan),)),
            pltpu.SemaphoreType.DMA((count + 2,)),
            pltpu.SemaphoreType.DMA((small,)),
            pltpu.SemaphoreType.DMA((small,)),
        ],
        compiler_params=pltpu.CompilerParams(collective_id=0, has_side_effects=True),
        name="gather_all",
    )(*own, rows, scales)
    whole = [g.reshape((shards,) + a.shape) for g, a in zip(result, arrays)]
    return whole, result[count], result[count + 1]


def layer_kernel(
    channels, length,
    residual, mixer_gain, value_scale, input_scale, output_scale, taps, conv_gain, channel_gain,
    gate_scale, up_scale, out_scale, down_scale,
    *refs,
):
    raw, out_ref, refs = refs[:7], refs[7], refs[8:]
    bufs, refs = refs[:5], refs[5:]
    others, refs = refs[:5], refs[5:]
    stages, refs = refs[:7], refs[7:]
    (own_res, own_scales, res, scales, gains, mixes, after, normed, gate_buf, hidden, outgoing, from_x, to_z, from_z, to_x, whole_z,
     raw_sem, z_send, z_recv, y_send, y_recv, t_send, t_recv, mx_send, mx_recv, mt_send, mt_recv,
     r_send, r_recv, s_send, s_recv, m_send, m_recv, px_send, px_recv, pz_send, pz_recv,
     zz_send, zz_recv) = refs
    proj_buf, mout_buf, gate_w, up_w, down_w = bufs
    shards = gate_w.shape[0]
    place = lax.axis_index("fs")
    core = lax.axis_index("rep")
    group = lax.axis_index("tp")
    own_width, tokens = residual.shape
    mix_scales = (value_scale, input_scale, output_scale)
    features = 2 * own_width
    block = mout_buf.shape[-1]
    per_group = shards // 2
    depth = shards // 2
    width = gate_w.shape[-1]
    narrow = mixes.shape[-1]
    all_tokens = 2 * tokens

    z, y = place // 2, place % 2
    side = z % 2
    part_of = ((z + 1) // 2) % 2
    high = (z * 2 + y) // per_group
    pair = z + 1 - 2 * side
    inner = part_of == 1
    outer = part_of == 0
    opposite = 1 - z // 2
    levels = [z, pair, 1 + opposite, (depth - 1) * opposite]
    twin = {"rep": 1 - core}
    across = {"fs": z * 2 + 1 - y}
    beside = {"tp": 1 - group}
    mate = {"fs": pair * 2 + y}
    corner = {"fs": pair * 2 + y, "tp": 1 - group}

    def remote(source, target, send, recv, device):
        return pltpu.make_async_remote_copy(
            source, target, send, recv, device_id=device, device_id_type=MESH
        )

    def spot(array, owner, half):
        if array == 1:
            return mout_buf.at[owner, group, half]
        if array >= 4:
            return down_w.at[owner, half, array - 4]
        return bufs[array].at[owner, half]

    def owner_of(r, far):
        return levels[r] * 2 + (1 - y if far else y)

    def z_copy(array, way):
        target = spot(array, pair * 2 + y if way == 4 else place, core)
        if array == 1 or way in (2, 4):
            source = target
        else:
            source = others[array - 1 if array else 0]
        level = (None, pair, depth - 1 - z, depth - 1 - pair, depth - 1 - z)[way]
        kind = (None, 0, 2 - part_of, 2 - part_of, 2)[way]
        return remote(
            source, target, z_send.at[array, way - 1], z_recv.at[array, kind],
            {"fs": level * 2 + y},
        )

    def z_wait(array, r):
        target = spot(array, owner_of(r, False), core)
        remote(
            target, target, z_send.at[array, r - 1], z_recv.at[array, r - 1], across
        ).wait_recv()

    def y_copy(array, r):
        target = spot(array, owner_of(r, False), core)
        return remote(target, target, y_send.at[array, r], y_recv.at[array, r], across)

    def t_copy(array, r, far):
        target = spot(array, owner_of(r, far), core)
        index = r + 4 * far
        return remote(target, target, t_send.at[array, index], t_recv.at[array, index], twin)

    def mx_copy(r, far):
        target = spot(1, owner_of(r, far), core)
        index = r + 4 * far
        return remote(target, target, mx_send.at[index], mx_recv.at[index], beside)

    def mt_copy(r, far):
        target = mout_buf.at[owner_of(r, far), 1 - group, core]
        index = r + 4 * far
        return remote(target, target, mt_send.at[index], mt_recv.at[index], twin)

    rows = stages[0].shape[0]
    tall = stages[6].shape[1]
    raw_copies = []
    for i in range(4):
        raw_copies.append([pltpu.make_async_copy(
            raw[i].at[pl.ds(pl.multiple_of(core * rows, rows), rows)], stages[i], raw_sem.at[i])])
    for i in range(4, 6):
        raw_copies.append([pltpu.make_async_copy(
            raw[i].at[pl.ds(pl.multiple_of(core * rows, rows), rows)], stages[i], raw_sem.at[i])])
    raw_copies.append([
        pltpu.make_async_copy(
            raw[6].at[pl.ds(pl.multiple_of(k * width + core * tall, 16), tall)],
            stages[6].at[k], raw_sem.at[6 + k])
        for k in range(2)
    ])
    for group_of in raw_copies:
        for copy in group_of:
            copy.start()

    for first in range(0, own_width, tokens):
        own_res[:, first : first + tokens] = residual[first : first + tokens, :].T
    own_scales[...] = jnp.concatenate(
        [out_scale[...], down_scale[...], conv_gain[...], jnp.zeros((5, block), jnp.float32)], axis=0
    )

    barrier = pltpu.get_barrier_semaphore()
    partners = [{"fs": lax.rem(place + step, shards)} for step in range(1, shards)]
    partners += [beside, corner, twin]
    for other in partners:
        pl.semaphore_signal(barrier, inc=1, device_id=other, device_id_type=MESH)
    pl.semaphore_wait(barrier, len(partners))

    scale_copies = [
        remote(own_scales, scales.at[place], s_send.at[step], s_recv.at[step],
               {"fs": lax.rem(place + step, shards)})
        for step in range(1, shards)
    ]
    scale_copies.append(remote(own_scales, gains.at[group], s_send.at[0], s_recv.at[0], beside))
    res_z = remote(own_res, res.at[side, group], r_send.at[0], r_recv.at[0], mate)
    res_x = remote(own_res, res.at[side, group], r_send.at[1], r_recv.at[1], beside)
    passed = res.at[1 - side, group]
    res_d = remote(passed, passed, r_send.at[2], r_recv.at[2], beside)

    def start_z(*pairs):
        for array, r in pairs:
            z_copy(array, r).start()

    def start_inner(*pairs):
        @pl.when(inner)
        def _():
            for array, way in pairs:
                z_copy(array, way).start()

    def start_outer(*pairs):
        @pl.when(outer)
        def _():
            for array, way in pairs:
                z_copy(array, way).start()

    def wait_raw(*indices):
        for i in indices:
            for copy in raw_copies[i]:
                copy.wait()

    def both(first, second, size):
        return [
            (first, pl.ds(pl.multiple_of(part_of * size, 128), size)),
            (second, pl.ds(pl.multiple_of((1 - part_of) * size, 128), size)),
        ]

    res_z.start()
    res_x.start()
    wait_raw(0, 1, 2)
    for i in range(3):
        for target, cols in both(proj_buf.at[place, core], others[0], narrow):
            target[:, i * narrow : (i + 1) * narrow] = stages[i][:, cols].astype(jnp.bfloat16)
    start_z((0, 1), (0, 2), (0, 3))
    y_copy(0, 0).start()
    t_copy(0, 0, False).start()
    wait_raw(3)
    mout_buf[place, group, core] = stages[3][...].astype(jnp.bfloat16)
    start_z((1, 1), (1, 2), (1, 3))
    y_copy(1, 0).start()
    mx_copy(0, False).start()
    t_copy(1, 0, False).start()
    for copy in scale_copies:
        copy.start()
    for array in (2, 3):
        wait_raw(array + 2)
        for target, cols in both(bufs[array].at[place, core], others[array - 1], width):
            target[...] = stages[array + 2][:, cols].astype(jnp.bfloat16)
        t_copy(array, 0, False).start()
        if array == 2:
            y_copy(2, 0).start()
            start_z((2, 1))
            start_inner((2, 2))
    wait_raw(6)
    short = tall // 2
    for k, array in ((0, 4), (1, 5)):
        lines = slice(k * short, (k + 1) * short)
        down_w[place, core, k] = stages[6][part_of, lines, :].astype(jnp.bfloat16)
        others[array - 1][...] = stages[6][1 - part_of, lines, :].astype(jnp.bfloat16)
    for array in (4, 5):
        t_copy(array, 0, False).start()
    res[side, group] = own_res[...]
    scales[place] = own_scales[...]
    gains[group] = own_scales[...]

    def take_z(array, r):
        z_wait(array, r)
        if r == 1 and array >= 2:
            start_inner((array, 4))
        y_copy(array, r).start()
        t_copy(array, r, False).start()
        if array == 1:
            mx_copy(r, False).start()

    def take_y(array, r):
        y_copy(array, r).wait_recv()
        t_copy(array, r, True).start()
        if array == 1:
            mx_copy(r, True).start()

    def run(items):
        for kind, array, r in items:
            if kind == "s":
                z_copy(array, r).start()
            elif kind == "o":
                y_copy(array, r).start()
            else:
                (take_z if kind == "z" else take_y)(array, r)

    def each(outer_items, inner_items):
        @pl.when(outer)
        def _():
            run(outer_items)

        @pl.when(inner)
        def _():
            run(inner_items)

    def finish(array):
        for far in (False, True):
            for r in range(4):
                t_copy(array, r, far).wait_recv()

    def scaled(squares, count):
        return lax.rsqrt(squares / count + epsilon)

    def normalize_side(s):
        floats = [res[s, k].astype(jnp.float32) for k in range(2)]
        squares = sum(jnp.sum(row * row, axis=1, keepdims=True) for row in floats)
        factor = scaled(squares, features)
        lines = pl.ds(pl.multiple_of(s * tokens, tokens), tokens)
        for k in range(2):
            cols = slice(k * own_width, (k + 1) * own_width)
            normed[lines, cols] = (
                res[s, k].astype(jnp.float32) * factor * mixer_gain[:, cols]
            ).astype(jnp.bfloat16)

    order = (1, 2, 3)
    take_z(0, 2)
    take_z(1, 2)
    res_z.wait_recv()
    res_d.start()
    start_inner((2, 3))
    start_outer((2, 2))
    take_z(0, 1)
    take_z(0, 3)
    y_copy(3, 0).start()
    y_copy(4, 0).start()
    res_x.wait_recv()
    normalize_side(side)
    for r in (0, 2, 1, 3):
        take_y(0, r)
    res_d.wait_recv()
    normalize_side(1 - side)
    finish(0)

    own_cols = pl.ds(pl.multiple_of(part_of * narrow, 128), narrow)

    def project(index):
        weight = proj_buf[:, :, :, index * narrow : (index + 1) * narrow].reshape(features, narrow)
        product = jnp.dot(normed[...], weight, preferred_element_type=jnp.float32)
        return product * mix_scales[index][:, own_cols]

    value = project(0)
    u = project(1) * value
    place_in = lax.rem(lax.broadcasted_iota(jnp.int32, u.shape, 0), length)
    one = jnp.where(place_in >= 1, pltpu.roll(u, 1, 0), 0.0)
    two = jnp.where(place_in >= 2, pltpu.roll(u, 2, 0), 0.0)
    conv = taps[2:3, own_cols] * u + taps[1:2, own_cols] * one + taps[0:1, own_cols] * two
    mixes[group, part_of] = (project(2) * conv).astype(jnp.bfloat16)
    mix_slot = mixes.at[group, part_of]
    mix_copies = [
        remote(mix_slot, mix_slot, m_send.at[i], m_recv.at[i], device)
        for i, device in enumerate((mate, beside, corner))
    ]
    for copy in mix_copies:
        copy.start()
    start_z((3, 1))
    start_outer((3, 2))
    start_z((4, 1), (5, 1))
    each(
        [("z", 1, 3), ("z", 2, 2), ("z", 1, 1), ("z", 2, 3), ("z", 2, 1)],
        [("z", 1, 1), ("z", 1, 3), ("z", 2, 2), ("z", 2, 1)],
    )
    start_inner((3, 2), (3, 3))
    y_copy(5, 0).start()
    for r in (0, 2, 1, 3):
        take_y(1, r)
    for far in (False, True):
        for r in range(4):
            mx_copy(r, far).wait_recv()
            mt_copy(r, far).start()
    for copy in scale_copies + mix_copies:
        copy.wait_recv()
    finish(1)
    for far in (False, True):
        for r in range(4):
            mt_copy(r, far).wait_recv()
    total = jnp.zeros((all_tokens, 1), jnp.float32)
    for k in range(2):
        for b in range(2):
            lines = mixes[k, b].astype(jnp.float32)
            total = total + jnp.sum(lines * lines, axis=1, keepdims=True)
    factor = scaled(total, channels)
    for k in range(2):
        for b in range(2):
            cols = slice((2 * k + b) * narrow, (2 * k + b + 1) * narrow)
            hidden[:, cols] = (
                mixes[k, b].astype(jnp.float32) * factor
                * gains[k, 2:3, b * narrow : (b + 1) * narrow]
            ).astype(jnp.bfloat16)
    squares = jnp.zeros((all_tokens, 1), jnp.float32)
    for s in range(shards):
        k, inside = s // per_group, (s % per_group) * block
        part = jnp.dot(
            hidden[:, : 4 * narrow], mout_buf[s].reshape(4 * narrow, block),
            preferred_element_type=jnp.float32,
        ) * scales[s, 0:1, :]
        base = res[:, k, :, inside : inside + block].reshape(all_tokens, block)
        row = (base.astype(jnp.float32) + part).astype(jnp.bfloat16)
        after[s] = row
        row = row.astype(jnp.float32)
        squares = squares + jnp.sum(row * row, axis=1, keepdims=True)
    factor = scaled(squares, features)
    for s in range(shards):
        cols = slice(s * block, (s + 1) * block)
        normed[:, cols] = (
            after[s].astype(jnp.float32) * factor * channel_gain[:, cols]
        ).astype(jnp.bfloat16)

    def tiles(body):
        tile = 256
        whole = width // tile

        @pl.loop(0, whole)
        def _(j):
            body(pl.multiple_of(j * tile, tile), tile)

        if width % tile:
            body(whole * tile, width % tile)

    def multiply(weights, start, size):
        weight = weights[:, :, :, pl.ds(start, size)].reshape(features, size)
        return jnp.dot(normed[...], weight, preferred_element_type=jnp.float32)

    def scale_at(scale, start, size):
        first = part_of * (width // 128) + start // 128
        lines = [scale[pl.ds(first + i, 1), :] for i in range(size // 128)]
        return jnp.concatenate(lines, axis=1)

    def gate_tile(start, size):
        gate_buf[:, pl.ds(start, size)] = multiply(gate_w, start, size) * scale_at(
            gate_scale, start, size
        )

    def up_tile(start, size):
        product = multiply(up_w, start, size) * scale_at(up_scale, start, size)
        gate = gate_buf[:, pl.ds(start, size)]
        hidden[:, pl.ds(start, size)] = (
            gate / (1.0 + jnp.exp(-gate)) * product
        ).astype(jnp.bfloat16)

    each([], [("z", 2, 3), ("z", 3, 1)])
    start_inner((4, 2), (5, 2))
    for r in (0,) + order:
        take_y(2, r)
    finish(2)
    tiles(gate_tile)
    each(
        [("z", 3, 2), ("z", 3, 3), ("s", 4, 2), ("s", 5, 2), ("z", 3, 1), ("z", 4, 1), ("z", 5, 1), ("y", 3, 0),
         ("y", 3, 2), ("y", 3, 3), ("y", 3, 1)],
        [("z", 3, 2), ("z", 3, 3), ("s", 4, 3), ("s", 5, 3), ("z", 4, 1), ("z", 5, 1), ("y", 3, 0), ("y", 3, 1),
         ("y", 3, 2), ("z", 4, 2), ("z", 5, 2), ("y", 3, 3)],
    )
    finish(3)
    tiles(up_tile)

    steps = [(r, far) for r in range(4) for far in (False, True)]

    def index_of(k):
        return owner_of(*steps[k])

    def mine(k):
        return (high == group) if k < per_group else (high != group)

    def slot_of(k):
        return lax.rem(index_of(k), per_group)

    def px_copy(k, which):
        who = 1 - side if which == 0 else side
        return remote(
            to_x.at[k] if k % 2 else outgoing.at[k, who], from_x.at[k, who], px_send.at[k, which], px_recv.at[k, which], beside
        )

    def pz_copy(k):
        i = slot_of(k)
        return remote(to_z.at[i], from_z.at[i], pz_send.at[i], pz_recv.at[i], mate)

    def zz_copy(k):
        s = index_of(k)
        return remote(outgoing.at[k, 1 - side], whole_z.at[s], zz_send.at[s], zz_recv.at[s], mate)

    def down(k):
        r, far = steps[k]
        for array in (4, 5):
            t_copy(array, r, far).wait_recv()
        s = index_of(k)
        weight = down_w[s].reshape(width, block)
        part = jnp.dot(hidden[...], weight, preferred_element_type=jnp.float32)
        part = (part * scales[s, 1:2, :]).astype(jnp.bfloat16)
        outgoing[k, 0] = part[:tokens]
        outgoing[k, 1] = part[tokens:]

        if k % 2:
            zz_copy(k).start()
            return

        @pl.when(jnp.logical_not(mine(k)))
        def _():
            px_copy(k, 0).start()
            px_copy(k, 1).start()

    def pass_on(k):
        if k % 2:
            zz_copy(k).wait_recv()

            @pl.when(jnp.logical_not(mine(k)))
            def _():
                to_x[k] = (
                    outgoing[k, side].astype(jnp.float32) + whole_z[index_of(k)].astype(jnp.float32)
                ).astype(jnp.bfloat16)
                px_copy(k, 1).start()

            return

        @pl.when(mine(k))
        def _():
            px_copy(k, 0).wait_recv()
            to_z[slot_of(k)] = (
                outgoing[k, 1 - side].astype(jnp.float32) + from_x[k, 1 - side].astype(jnp.float32)
            ).astype(jnp.bfloat16)
            pz_copy(k).start()

    def close(k):
        i = slot_of(k)
        s = index_of(k)

        @pl.when(mine(k))
        def _():
            px_copy(k, 1).wait_recv()
            if k % 2 == 0:
                pz_copy(k).wait_recv()
            lines = pl.ds(pl.multiple_of(side * tokens, tokens), tokens)
            total = outgoing[k, side].astype(jnp.float32) + from_x[k, side].astype(jnp.float32)
            total = total + (whole_z[s] if k % 2 else from_z[i]).astype(jnp.float32)
            out_ref[:, pl.ds(pl.multiple_of(i * block, block), block)] = (
                after[s, lines, :].astype(jnp.float32) + total
            ).astype(jnp.bfloat16)

    def take_all(take, r):
        for array in (4, 5):
            take(array, r)

    each([("z", 4, 2), ("z", 5, 2)], [])
    down(0)
    take_all(take_y, 0)
    down(1)
    down(2)
    take_all(take_y, 1)
    down(3)
    down(4)
    take_all(take_z, 3)
    pass_on(1)
    take_all(take_y, 2)
    down(5)
    down(6)
    pass_on(3)
    pass_on(0)
    pass_on(4)
    pass_on(5)
    take_all(take_y, 3)
    down(7)
    pass_on(6)
    pass_on(2)
    pass_on(7)
    for k in range(shards):
        close(k)

    z_copy(0, 3).wait_send()
    z_copy(1, 3).wait_send()

    @pl.when(inner)
    def _():
        for array in range(2, 6):
            for way in (3, 4):
                z_copy(array, way).wait_send()

    for array in range(6):
        for r in range(4):
            if r in (1, 2):
                z_copy(array, r).wait_send()
            y_copy(array, r).wait_send()
            for far in (False, True):
                t_copy(array, r, far).wait_send()
    for r in range(4):
        for far in (False, True):
            mx_copy(r, far).wait_send()
            mt_copy(r, far).wait_send()
    for copy in scale_copies + mix_copies + [res_z, res_x, res_d]:
        copy.wait_send()
    for k in range(shards):
        if k % 2:
            zz_copy(k).wait_send()
        else:
            pl.when(mine(k))(pz_copy(k).wait_send)

        @pl.when(jnp.logical_not(mine(k)))
        def _():
            if k % 2 == 0:
                px_copy(k, 0).wait_send()
            px_copy(k, 1).wait_send()


def fused(
    shards, residual, small, raw,
):
    own_width, tokens = residual.shape
    features = 2 * own_width
    short = jnp.bfloat16
    in_rows, mix_width = raw[0].shape
    rows, narrow = in_rows // 2, mix_width // 2
    ff = raw[4].shape[1]
    width = ff // 2
    out_rows, block = raw[3].shape
    channels = 2 * out_rows
    tall = width // 2
    steps = shards
    vmem = pl.BlockSpec(memory_space=pltpu.VMEM)
    dma = pltpu.SemaphoreType.DMA
    return pl.pallas_call(
        functools.partial(layer_kernel, channels, LEN),
        out_shape=jax.ShapeDtypeStruct((tokens, own_width), short),
        in_specs=[vmem] * (1 + len(small)) + [pl.BlockSpec(memory_space=pl.ANY)] * 7,
        out_specs=vmem,
        scratch_shapes=[
            pltpu.VMEM((shards, 2, rows, 3 * narrow), short),
            pltpu.VMEM((shards, 2, 2, out_rows // 2, block), short),
            pltpu.VMEM((shards, 2, rows, width), short),
            pltpu.VMEM((shards, 2, rows, width), short),
            pltpu.VMEM((shards, 2, 2, tall // 2, block), short),
            pltpu.VMEM((rows, 3 * narrow), short),
            pltpu.VMEM((rows, width), short),
            pltpu.VMEM((rows, width), short),
            pltpu.VMEM((tall // 2, block), short),
            pltpu.VMEM((tall // 2, block), short),
        ]
        + [pltpu.VMEM((rows, mix_width), jnp.float32)] * 3
        + [
            pltpu.VMEM((out_rows // 2, block), jnp.float32),
            pltpu.VMEM((rows, ff), jnp.float32),
            pltpu.VMEM((rows, ff), jnp.float32),
            pltpu.VMEM((2, tall, block), jnp.float32),
            pltpu.VMEM((tokens, own_width), short),
            pltpu.VMEM((8, block), jnp.float32),
            pltpu.VMEM((2, 2, tokens, own_width), short),
            pltpu.VMEM((shards, 8, block), jnp.float32),
            pltpu.VMEM((2, 8, block), jnp.float32),
            pltpu.VMEM((2, 2, 2 * tokens, narrow), short),
            pltpu.VMEM((shards, 2 * tokens, block), short),
            pltpu.VMEM((2 * tokens, features), short),
            pltpu.VMEM((2 * tokens, width), jnp.float32),
            pltpu.VMEM((2 * tokens, width), short),
            pltpu.VMEM((steps, 2, tokens, block), short),
            pltpu.VMEM((steps, 2, tokens, block), short),
            pltpu.VMEM((steps // 2, tokens, block), short),
            pltpu.VMEM((steps // 2, tokens, block), short),
            pltpu.VMEM((steps, tokens, block), short),
            pltpu.VMEM((steps, tokens, block), short),
            dma((8,)),
            dma((6, 4)),
            dma((6, 3)),
            dma((6, 4)),
            dma((6, 4)),
            dma((6, 8)),
            dma((6, 8)),
            dma((8,)),
            dma((8,)),
            dma((8,)),
            dma((8,)),
            dma((3,)),
            dma((3,)),
            dma((shards,)),
            dma((shards,)),
            dma((3,)),
            dma((3,)),
            dma((steps, 2)),
            dma((steps, 2)),
            dma((steps // 2,)),
            dma((steps // 2,)),
            dma((steps,)),
            dma((steps,)),
        ],
        compiler_params=pltpu.CompilerParams(
            collective_id=1, has_side_effects=True, vmem_limit_bytes=60 * 1024 * 1024
        ),
        name="layer",
    )(
        residual, *small, *raw,
    )


def local(
    reps,
    shards,
    groups,
    residual,
    mixer_gain,
    value_weight,
    value_scale,
    input_gate_weight,
    input_gate_scale,
    output_gate_weight,
    output_gate_scale,
    conv_taps,
    conv_gain,
    mixer_out_weight,
    mixer_out_scale,
    channel_gain,
    gate_weight,
    gate_scale,
    up_weight,
    up_scale,
    down_weight,
    down_scale,
):
    own_rows, tokens = residual.shape
    width = value_weight.shape[1]
    channels = width * groups
    features = own_rows * groups
    short = jnp.bfloat16
    block, ff = mixer_out_weight.shape[1], gate_weight.shape[1]
    in_rows, out_rows = value_weight.shape[0], mixer_out_weight.shape[0]
    if (
        reps == 2 and groups == 2 and shards == 8 and tokens % LEN == 0
        and block % 128 == 0 and width % 256 == 0 and ff % 256 == 0 and block == width
        and in_rows % 32 == 0 and out_rows == width and own_rows == block * shards // 2
    ):
        result = fused(
            shards, residual,
            [mixer_gain[None], value_scale[None], input_gate_scale[None], output_gate_scale[None],
             conv_taps, conv_gain[None], channel_gain[None], gate_scale.reshape(-1, 128),
             up_scale.reshape(-1, 128), mixer_out_scale[None], down_scale[None]],
            [value_weight, input_gate_weight, output_gate_weight, mixer_out_weight,
             gate_weight, up_weight, down_weight],
        )
        return result.T
    projections = jnp.concatenate(
        [value_weight.astype(short), input_gate_weight.astype(short), output_gate_weight.astype(short)],
        axis=1,
    )
    arrays = [
        projections,
        mixer_out_weight.astype(short),
        gate_weight.astype(short),
        up_weight.astype(short),
        down_weight.astype(short),
    ]
    scales = jnp.stack([mixer_out_scale, down_scale])
    (proj_all, out_all, gate_all, up_all, down_all), rows_all, scales_all = gather_all(
        arrays, residual, scales, groups, shards, reps
    )
    whole = rows_all.reshape(features, tokens)
    out_scale = scales_all[:, 0].reshape(features)
    down_scale_full = scales_all[:, 1].reshape(features)

    normed = normalize(whole, mixer_gain)
    projected = contract(proj_all.reshape(features, 3 * width), normed)
    value = projected[:width] * value_scale[:, None]
    in_gate = projected[width : 2 * width] * input_gate_scale[:, None]
    out_gate = projected[2 * width :] * output_gate_scale[:, None]
    mixed = out_gate * causal_conv(in_gate * value, conv_taps, LEN)
    squares = lax.psum(jnp.sum(mixed * mixed, axis=0), "tp")
    conv_normed = (
        mixed * lax.rsqrt(squares / channels + epsilon)[None, :] * conv_gain[:, None]
    ).astype(short)
    part = lax.dot_general(
        out_all, conv_normed, (((1,), (0,)), ((), ())), preferred_element_type=jnp.float32
    ).reshape(features, tokens)
    rounded = (part * out_scale[:, None]).astype(short)
    parts = lax.all_gather(rounded, "tp", axis=0)
    total = jnp.sum(parts.astype(jnp.float32), axis=0)
    after_whole = (whole.astype(jnp.float32) + total).astype(short)
    after_own = lax.dynamic_slice_in_dim(
        after_whole, lax.axis_index("tp") * own_rows, own_rows, 0
    )
    normed_two = normalize(after_whole, channel_gain)
    gate = contract(gate_all.reshape(features, -1), normed_two)
    upper = contract(up_all.reshape(features, -1), normed_two)
    hidden = (jax.nn.silu(gate * gate_scale[:, None]) * (upper * up_scale[:, None])).astype(short)
    down = lax.dot_general(
        down_all, hidden, (((1,), (0,)), ((), ())), preferred_element_type=jnp.float32
    ).reshape(features, tokens)
    total_two = lax.psum_scatter(
        (down * down_scale_full[:, None]).astype(short),
        "tp",
        scatter_dimension=0,
        tiled=True,
    ).astype(jnp.float32)
    return (after_own.astype(jnp.float32) + total_two).astype(short)


def solution(mesh):
    placed = (
        P("tp", ("rep", "fs")),
        P(),
        P("fs", "tp"),
        P("tp"),
        P("fs", "tp"),
        P("tp"),
        P("fs", "tp"),
        P("tp"),
        P(None, "tp"),
        P("tp"),
        P("tp", "fs"),
        P("fs"),
        P(),
        P("fs", "tp"),
        P("tp"),
        P("fs", "tp"),
        P("tp"),
        P("tp", "fs"),
        P("fs"),
    )
    sizes = mesh.shape["rep"], mesh.shape["fs"], mesh.shape["tp"]
    return jax.shard_map(
        functools.partial(local, *sizes),
        mesh=mesh,
        in_specs=placed,
        out_specs=P("tp", ("rep", "fs")),
        check_vma=False,
    )
```

```python
import functools

import jax
import jax.numpy as jnp
from jax import lax
from jax.experimental import pallas as pl
from jax.experimental.pallas import tpu as pltpu
from jax.sharding import PartitionSpec as P

LEN = 128
MESH = pl.DeviceIdType.MESH

epsilon = 1e-06


def contract(weight, rows):
    return lax.dot_general(
        weight, rows, (((0,), (0,)), ((), ())), preferred_element_type=jnp.float32
    )


def normalize(values, gain):
    floats = values.astype(jnp.float32)
    mean = jnp.mean(floats * floats, axis=0, keepdims=True)
    return (floats * lax.rsqrt(mean + epsilon) * gain[:, None]).astype(jnp.bfloat16)


def causal_conv(values, taps, length):
    total = values.shape[1]
    position = jnp.arange(total, dtype=jnp.int32) % length
    shifted_one = jnp.pad(values, ((0, 0), (1, 0)))[:, :total]
    shifted_two = jnp.pad(values, ((0, 0), (2, 0)))[:, :total]
    shifted_one = jnp.where(position[None, :] >= 1, shifted_one, 0.0)
    shifted_two = jnp.where(position[None, :] >= 2, shifted_two, 0.0)
    return (
        taps[2][:, None] * values + taps[1][:, None] * shifted_one + taps[0][:, None] * shifted_two
    )


def ring_plan(sizes, ring):
    free = {"up": 0.0, "down": 0.0, "y": 0.0, "d": 0.0}
    rate = {"up": 46.0, "down": 46.0, "y": 46.0, "d": 330.0}
    waiting = []
    for array in range(len(sizes)):
        for chunk in range(4):
            waiting.append((0.0, array, chunk, 0, 0, None))
    order = []
    pending = []

    def push(ready, send, link, needs):
        pending.append((ready, send, link, needs))

    def ahead(ready, array, chunk, pair, hop, needs):
        link = "up" if chunk % 2 == 0 else "down"
        if hop < ring - 1:
            push(ready, (array, chunk, pair, hop, "z"), link, needs)
        if chunk < 2 and pair == 0 and hop == 0:
            push(ready, (array, chunk, pair, hop, "y"), "y", needs)
        if chunk >= 2 and pair == 0:
            push(ready, (array, chunk, pair, hop, "y"), "y", needs)
        if needs is not None:
            push(ready, (array, chunk, pair, hop, "d"), "d", needs)

    for _, array, chunk, pair, hop, needs in waiting:
        ahead(0.0, array, chunk, pair, hop, needs)
    while pending:
        best = min(
            range(len(pending)),
            key=lambda i: (
                max(pending[i][0], free[pending[i][2]]),
                pending[i][1][0],
                pending[i][0],
                i,
            ),
        )
        ready, send, link, needs = pending.pop(best)
        begin = max(ready, free[link])
        end = begin + sizes[send[0]] / rate[link] / 1e3
        free[link] = end
        order.append((begin, ready, send, needs))
        array, chunk, pair, hop, kind = send
        if kind == "z":
            ahead(end + 2.0, array, chunk, pair, hop + 1, send)
        elif kind == "y":
            if chunk < 2:
                ahead(end + 2.0, array, chunk, 1, 0, send)
            else:
                push(end + 2.0, (array, chunk, 1, hop, "d"), "d", send)
    order.sort(key=lambda item: item[1])
    return [(send, needs) for _, _, send, needs in order]


def gather_kernel(plan, count, groups, shards, *refs):
    own, (own_rows, own_scales) = refs[:count], refs[count : count + 2]
    outs = refs[count + 2 : 2 * count + 2]
    out_rows, out_scales = refs[2 * count + 2 : 2 * count + 4]
    send_sem, recv_sem, local_sem, small_send, small_recv = refs[2 * count + 4 :]
    ring = shards // 2
    place = lax.axis_index("fs")
    core = lax.axis_index("rep")
    group = lax.axis_index("tp")
    z, y = place // 2, place % 2
    up = {"fs": lax.rem(z + 1, ring) * 2 + y}
    down = {"fs": lax.rem(z + ring - 1, ring) * 2 + y}
    across = {"fs": z * 2 + (1 - y)}
    twin = {"rep": 1 - core}

    barrier = pltpu.get_barrier_semaphore()
    others = [{"fs": lax.rem(place + step, shards)} for step in range(1, shards)]
    others += [{"tp": lax.rem(group + step, groups)} for step in range(1, groups)]
    others += [twin]
    for other in others:
        pl.semaphore_signal(barrier, inc=1, device_id=other, device_id_type=MESH)
    pl.semaphore_wait(barrier, len(others))

    small = []
    for step in range(1, groups):
        small.append(
            pltpu.make_async_remote_copy(
                own_rows, out_rows.at[group], small_send.at[step - 1], small_recv.at[step - 1],
                device_id={"tp": lax.rem(group + step, groups)}, device_id_type=MESH,
            )
        )
    for step in range(1, shards):
        index = groups - 1 + step - 1
        small.append(
            pltpu.make_async_remote_copy(
                own_scales, out_scales.at[place], small_send.at[index], small_recv.at[index],
                device_id={"fs": lax.rem(place + step, shards)}, device_id_type=MESH,
            )
        )
    for copy in small:
        copy.start()

    copies = {}
    for number, (send, _) in enumerate(plan):
        array, chunk, pair, hop, kind = send
        step = hop if chunk % 2 == 0 else ring - hop
        owner = lax.rem(z + ring - step, ring) * 2 + (y if pair == 0 else 1 - y)
        slot = outs[array].at[owner, core, chunk]
        source = own[array].at[core, chunk] if (hop == 0 and pair == 0) else slot
        target = {"z": up if chunk % 2 == 0 else down, "y": across, "d": twin}[kind]
        copies[send] = pltpu.make_async_remote_copy(
            source, slot, send_sem.at[number], recv_sem.at[number],
            device_id=target, device_id_type=MESH,
        )

    local = [
        pltpu.make_async_copy(own[array], outs[array].at[place], local_sem.at[array])
        for array in range(count)
    ]
    local.append(pltpu.make_async_copy(own_rows, out_rows.at[group], local_sem.at[count]))
    local.append(pltpu.make_async_copy(own_scales, out_scales.at[place], local_sem.at[count + 1]))

    arrived = set()
    started_local = False
    for send, needs in plan:
        if needs is not None and needs not in arrived:
            if not started_local:
                started_local = True
                for copy in local:
                    copy.start()
            copies[needs].wait_recv()
            arrived.add(needs)
        copies[send].start()
    for send, _ in plan:
        copies[send].wait_send()
        if send not in arrived:
            copies[send].wait_recv()
    for copy in small:
        copy.wait()
    for copy in local:
        copy.wait()


def gather_all(arrays, rows, scales, groups, shards, reps):
    count = len(arrays)
    own = [a.reshape(reps, 4, a.shape[0] // (4 * reps), a.shape[1]) for a in arrays]
    sizes = [a.size // (4 * reps) * a.dtype.itemsize for a in arrays]
    plan = ring_plan(sizes, shards // 2)
    small = groups - 1 + shards - 1
    result = pl.pallas_call(
        functools.partial(gather_kernel, plan, count, groups, shards),
        out_shape=[jax.ShapeDtypeStruct((shards,) + a.shape, a.dtype) for a in own]
        + [
            jax.ShapeDtypeStruct((groups,) + rows.shape, rows.dtype),
            jax.ShapeDtypeStruct((shards,) + scales.shape, scales.dtype),
        ],
        in_specs=[pl.BlockSpec(memory_space=pl.ANY)] * (count + 2),
        out_specs=[pl.BlockSpec(memory_space=pl.ANY)] * (count + 2),
        scratch_shapes=[
            pltpu.SemaphoreType.DMA((len(plan),)),
            pltpu.SemaphoreType.DMA((len(plan),)),
            pltpu.SemaphoreType.DMA((count + 2,)),
            pltpu.SemaphoreType.DMA((small,)),
            pltpu.SemaphoreType.DMA((small,)),
        ],
        compiler_params=pltpu.CompilerParams(collective_id=0, has_side_effects=True),
        name="gather_all",
    )(*own, rows, scales)
    whole = [g.reshape((shards,) + a.shape) for g, a in zip(result, arrays)]
    return whole, result[count], result[count + 1]


def layer_kernel(
    channels, length,
    residual, mixer_gain, value_scale, input_scale, output_scale, taps, conv_gain, channel_gain,
    gate_scale, up_scale, out_scale, down_scale,
    *refs,
):
    raw, out_ref, refs = refs[:7], refs[7], refs[8:]
    bufs, refs = refs[:5], refs[5:]
    others, refs = refs[:7], refs[7:]
    stages, refs = refs[:7], refs[7:]
    (own_res, own_scales, res, scales, gains, mixes, after, normed, gate_buf, hidden, outgoing, from_x, to_z, from_z, to_x, whole_z, out_buf,
     raw_sem, z_send, z_recv, y_send, y_recv, t_send, t_recv, mx_send, mx_recv, mt_send, mt_recv,
     r_send, r_recv, s_send, s_recv, m_send, m_recv, px_send, px_recv, pz_send, pz_recv,
     zz_send, zz_recv, out_sem) = refs
    proj_buf, mout_buf, gate_w, up_w, down_w = bufs
    shards = gate_w.shape[0]
    place = lax.axis_index("fs")
    core = lax.axis_index("rep")
    group = lax.axis_index("tp")
    own_width, tokens = residual.shape
    mix_scales = (value_scale, input_scale, output_scale)
    features = 2 * own_width
    block = mout_buf.shape[-1]
    per_group = shards // 2
    depth = shards // 2
    width = gate_w.shape[-1]
    narrow = mixes.shape[-1]
    all_tokens = 2 * tokens

    z, y = place // 2, place % 2
    side = z % 2
    part_of = ((z + 1) // 2) % 2
    high = (z * 2 + y) // per_group
    pair = z + 1 - 2 * side
    inner = part_of == 1
    outer = part_of == 0
    opposite = 1 - z // 2
    levels = [z, pair, 1 + opposite, (depth - 1) * opposite]
    twin = {"rep": 1 - core}
    across = {"fs": z * 2 + 1 - y}
    beside = {"tp": 1 - group}
    mate = {"fs": pair * 2 + y}
    corner = {"fs": pair * 2 + y, "tp": 1 - group}

    def remote(source, target, send, recv, device):
        return pltpu.make_async_remote_copy(
            source, target, send, recv, device_id=device, device_id_type=MESH
        )

    def spot(array, owner, half):
        if array == 1:
            return mout_buf.at[owner, group, half]
        if array >= 2:
            return bufs[1 + array // 2].at[owner, half, array % 2]
        return proj_buf.at[owner, half]

    def owner_of(r, far):
        return levels[r] * 2 + (1 - y if far else y)

    def z_copy(array, way):
        target = spot(array, pair * 2 + y if way == 4 else place, core)
        if array == 1 or way in (2, 4):
            source = target
        else:
            source = others[array - 1 if array else 0]
        level = (None, pair, depth - 1 - z, depth - 1 - pair, depth - 1 - z)[way]
        kind = (None, 0, 2 - part_of, 2 - part_of, 2)[way]
        return remote(
            source, target, z_send.at[array, way - 1], z_recv.at[array, kind],
            {"fs": level * 2 + y},
        )

    def z_wait(array, r):
        target = spot(array, owner_of(r, False), core)
        remote(
            target, target, z_send.at[array, r - 1], z_recv.at[array, r - 1], across
        ).wait_recv()

    def y_copy(array, r):
        target = spot(array, owner_of(r, False), core)
        return remote(target, target, y_send.at[array, r], y_recv.at[array, r], across)

    def t_copy(array, r, far):
        target = spot(array, owner_of(r, far), core)
        index = r + 4 * far
        return remote(target, target, t_send.at[array, index], t_recv.at[array, index], twin)

    def mx_copy(r, far):
        target = spot(1, owner_of(r, far), core)
        index = r + 4 * far
        return remote(target, target, mx_send.at[index], mx_recv.at[index], beside)

    def mt_copy(r, far):
        target = mout_buf.at[owner_of(r, far), 1 - group, core]
        index = r + 4 * far
        return remote(target, target, mt_send.at[index], mt_recv.at[index], twin)

    rows = stages[0].shape[0]
    tall = stages[6].shape[1]
    raw_copies = []
    for i in range(4):
        raw_copies.append([pltpu.make_async_copy(
            raw[i].at[pl.ds(pl.multiple_of(core * rows, rows), rows)], stages[i], raw_sem.at[i])])
    for i in range(4, 6):
        raw_copies.append([pltpu.make_async_copy(
            raw[i].at[pl.ds(pl.multiple_of(core * rows, rows), rows)], stages[i], raw_sem.at[i])])
    raw_copies.append([
        pltpu.make_async_copy(
            raw[6].at[pl.ds(pl.multiple_of(k * width + core * tall, 16), tall)],
            stages[6].at[k], raw_sem.at[6 + k])
        for k in range(2)
    ])
    for group_of in raw_copies:
        for copy in group_of:
            copy.start()

    for first in range(0, own_width, tokens):
        own_res[:, first : first + tokens] = residual[first : first + tokens, :].T
    own_scales[...] = jnp.concatenate(
        [out_scale[...], down_scale[...], conv_gain[...], jnp.zeros((5, block), jnp.float32)], axis=0
    )

    barrier = pltpu.get_barrier_semaphore()
    partners = [{"fs": lax.rem(place + step, shards)} for step in range(1, shards)]
    partners += [beside, corner, twin]
    for other in partners:
        pl.semaphore_signal(barrier, inc=1, device_id=other, device_id_type=MESH)
    pl.semaphore_wait(barrier, len(partners))

    scale_copies = [
        remote(own_scales, scales.at[place], s_send.at[step], s_recv.at[step],
               {"fs": lax.rem(place + step, shards)})
        for step in range(1, shards)
    ]
    scale_copies.append(remote(own_scales, gains.at[group], s_send.at[0], s_recv.at[0], beside))
    res_z = remote(own_res, res.at[side, group], r_send.at[0], r_recv.at[0], mate)
    res_x = remote(own_res, res.at[side, group], r_send.at[1], r_recv.at[1], beside)
    passed = res.at[1 - side, group]
    res_d = remote(passed, passed, r_send.at[2], r_recv.at[2], beside)

    def start_z(*pairs):
        for array, r in pairs:
            z_copy(array, r).start()

    def start_inner(*pairs):
        @pl.when(inner)
        def _():
            for array, way in pairs:
                z_copy(array, way).start()

    def start_outer(*pairs):
        @pl.when(outer)
        def _():
            for array, way in pairs:
                z_copy(array, way).start()

    def wait_raw(*indices):
        for i in indices:
            for copy in raw_copies[i]:
                copy.wait()

    def both(first, second, size):
        return [
            (first, pl.ds(pl.multiple_of(part_of * size, 128), size)),
            (second, pl.ds(pl.multiple_of((1 - part_of) * size, 128), size)),
        ]

    res_z.start()
    res_x.start()
    wait_raw(0, 1, 2)
    for i in range(3):
        for target, cols in both(proj_buf.at[place, core], others[0], narrow):
            target[:, i * narrow : (i + 1) * narrow] = stages[i][:, cols].astype(jnp.bfloat16)
    start_z((0, 1), (0, 2), (0, 3))
    y_copy(0, 0).start()
    t_copy(0, 0, False).start()
    wait_raw(3)
    mout_buf[place, group, core] = stages[3][...].astype(jnp.bfloat16)
    start_z((1, 1), (1, 2), (1, 3))
    y_copy(1, 0).start()
    mx_copy(0, False).start()
    t_copy(1, 0, False).start()
    for copy in scale_copies:
        copy.start()
    fine = rows // 2
    for matrix in (1, 2):
        wait_raw(matrix + 3)
        for chunk in range(2):
            array = 2 * matrix + chunk
            lines = slice(chunk * fine, (chunk + 1) * fine)
            for target, cols in both(spot(array, place, core), others[array - 1], width):
                target[...] = stages[matrix + 3][lines, cols].astype(jnp.bfloat16)
            t_copy(array, 0, False).start()
            if matrix == 1:
                y_copy(array, 0).start()
                start_outer((array, 1))
                start_inner((array, 2))
    wait_raw(6)
    short = tall // 2
    for chunk in range(2):
        array = 6 + chunk
        lines = slice(chunk * short, (chunk + 1) * short)
        down_w[place, core, chunk] = stages[6][part_of, lines, :].astype(jnp.bfloat16)
        others[array - 1][...] = stages[6][1 - part_of, lines, :].astype(jnp.bfloat16)
        t_copy(array, 0, False).start()
    res[side, group] = own_res[...]
    scales[place] = own_scales[...]
    gains[group] = own_scales[...]

    def take_z(array, r):
        z_wait(array, r)
        if r == 1 and array >= 2:
            start_inner((array, 4))
        y_copy(array, r).start()
        t_copy(array, r, False).start()
        if array == 1:
            mx_copy(r, False).start()

    def take_y(array, r):
        y_copy(array, r).wait_recv()
        t_copy(array, r, True).start()
        if array == 1:
            mx_copy(r, True).start()

    def run(items):
        for kind, array, r in items:
            if kind == "s":
                z_copy(array, r).start()
            elif kind == "o":
                y_copy(array, r).start()
            else:
                (take_z if kind == "z" else take_y)(array, r)

    def each(outer_items, inner_items):
        @pl.when(outer)
        def _():
            run(outer_items)

        @pl.when(inner)
        def _():
            run(inner_items)

    def finish(array):
        for far in (False, True):
            for r in range(4):
                t_copy(array, r, far).wait_recv()

    def scaled(squares, count):
        return lax.rsqrt(squares / count + epsilon)

    def normalize_side(s):
        floats = [res[s, k].astype(jnp.float32) for k in range(2)]
        squares = sum(jnp.sum(row * row, axis=1, keepdims=True) for row in floats)
        factor = scaled(squares, features)
        lines = pl.ds(pl.multiple_of(s * tokens, tokens), tokens)
        for k in range(2):
            cols = slice(k * own_width, (k + 1) * own_width)
            normed[lines, cols] = (
                res[s, k].astype(jnp.float32) * factor * mixer_gain[:, cols]
            ).astype(jnp.bfloat16)

    order = (1, 2, 3)
    take_z(0, 2)
    take_z(1, 2)
    for array in (4, 5):
        y_copy(array, 0).start()
    res_z.wait_recv()
    res_d.start()
    start_inner((2, 3), (3, 3))
    start_outer((2, 2), (3, 2))
    take_z(0, 1)
    take_z(0, 3)
    for array in (6, 7):
        y_copy(array, 0).start()
    res_x.wait_recv()
    normalize_side(side)
    for r in (0, 2, 1, 3):
        take_y(0, r)
    res_d.wait_recv()
    normalize_side(1 - side)
    finish(0)

    own_cols = pl.ds(pl.multiple_of(part_of * narrow, 128), narrow)

    def project(index):
        weight = proj_buf[:, :, :, index * narrow : (index + 1) * narrow].reshape(features, narrow)
        product = jnp.dot(normed[...], weight, preferred_element_type=jnp.float32)
        return product * mix_scales[index][:, own_cols]

    value = project(0)
    u = project(1) * value
    place_in = lax.rem(lax.broadcasted_iota(jnp.int32, u.shape, 0), length)
    one = jnp.where(place_in >= 1, pltpu.roll(u, 1, 0), 0.0)
    two = jnp.where(place_in >= 2, pltpu.roll(u, 2, 0), 0.0)
    conv = taps[2:3, own_cols] * u + taps[1:2, own_cols] * one + taps[0:1, own_cols] * two
    mixes[group, part_of] = (project(2) * conv).astype(jnp.bfloat16)
    mix_slot = mixes.at[group, part_of]
    mix_copies = [
        remote(mix_slot, mix_slot, m_send.at[i], m_recv.at[i], device)
        for i, device in enumerate((mate, beside, corner))
    ]
    for copy in mix_copies:
        copy.start()
    start_inner((2, 1), (3, 1))
    start_z((4, 1), (5, 1))
    start_outer((4, 2), (5, 2))
    start_z((6, 1), (7, 1))
    each(
        [("z", 1, 3), ("z", 2, 2), ("z", 2, 3), ("z", 1, 1), ("z", 3, 2), ("z", 3, 3)],
        [("z", 1, 1), ("z", 1, 3), ("z", 2, 2), ("z", 3, 2), ("z", 2, 1), ("z", 3, 1),
         ("s", 4, 2), ("s", 4, 3), ("s", 5, 2), ("s", 5, 3)],
    )
    for r in (0, 2, 1, 3):
        take_y(1, r)
    for far in (False, True):
        for r in range(4):
            mx_copy(r, far).wait_recv()
            mt_copy(r, far).start()
    for copy in scale_copies + mix_copies:
        copy.wait_recv()
    finish(1)
    for far in (False, True):
        for r in range(4):
            mt_copy(r, far).wait_recv()
    total = jnp.zeros((all_tokens, 1), jnp.float32)
    for k in range(2):
        for b in range(2):
            lines = mixes[k, b].astype(jnp.float32)
            total = total + jnp.sum(lines * lines, axis=1, keepdims=True)
    factor = scaled(total, channels)
    for k in range(2):
        for b in range(2):
            cols = slice((2 * k + b) * narrow, (2 * k + b + 1) * narrow)
            hidden[:, cols] = (
                mixes[k, b].astype(jnp.float32) * factor
                * gains[k, 2:3, b * narrow : (b + 1) * narrow]
            ).astype(jnp.bfloat16)
    squares = jnp.zeros((all_tokens, 1), jnp.float32)
    for s in range(shards):
        k, inside = s // per_group, (s % per_group) * block
        part = jnp.dot(
            hidden[:, : 4 * narrow], mout_buf[s].reshape(4 * narrow, block),
            preferred_element_type=jnp.float32,
        ) * scales[s, 0:1, :]
        base = res[:, k, :, inside : inside + block].reshape(all_tokens, block)
        row = (base.astype(jnp.float32) + part).astype(jnp.bfloat16)
        after[s] = row
        row = row.astype(jnp.float32)
        squares = squares + jnp.sum(row * row, axis=1, keepdims=True)
    factor = scaled(squares, features)
    for s in range(shards):
        cols = slice(s * block, (s + 1) * block)
        normed[:, cols] = (
            after[s].astype(jnp.float32) * factor * channel_gain[:, cols]
        ).astype(jnp.bfloat16)

    def tiles(body):
        tile = 256
        whole = width // tile

        @pl.loop(0, whole)
        def _(j):
            body(pl.multiple_of(j * tile, tile), tile)

        if width % tile:
            body(whole * tile, width % tile)

    def multiply(weights, start, size):
        weight = weights[:, :, :, :, pl.ds(start, size)].reshape(features, size)
        return jnp.dot(normed[...], weight, preferred_element_type=jnp.float32)

    def scale_at(scale, start, size):
        first = part_of * (width // 128) + start // 128
        lines = [scale[pl.ds(first + i, 1), :] for i in range(size // 128)]
        return jnp.concatenate(lines, axis=1)

    def gate_tile(start, size):
        gate_buf[:, pl.ds(start, size)] = multiply(gate_w, start, size) * scale_at(
            gate_scale, start, size
        )

    def up_tile(start, size):
        product = multiply(up_w, start, size) * scale_at(up_scale, start, size)
        gate = gate_buf[:, pl.ds(start, size)]
        hidden[:, pl.ds(start, size)] = (
            gate / (1.0 + jnp.exp(-gate)) * product
        ).astype(jnp.bfloat16)

    each(
        [("z", 2, 1), ("z", 3, 1), ("z", 4, 2), ("z", 4, 3)],
        [("z", 2, 3), ("z", 3, 3), ("z", 4, 1), ("z", 5, 1), ("s", 6, 2), ("s", 7, 2)],
    )
    for array in (2, 3):
        for r in (0,) + order:
            take_y(array, r)
    finish(2)
    finish(3)
    tiles(gate_tile)
    each(
        [("z", 5, 2), ("z", 5, 3), ("s", 6, 2), ("s", 7, 2),
         ("z", 4, 1), ("z", 5, 1), ("z", 6, 1), ("z", 7, 1),
         ("y", 4, 0), ("y", 5, 0), ("y", 4, 2), ("y", 4, 3), ("y", 5, 2), ("y", 5, 3),
         ("y", 4, 1), ("y", 5, 1)],
        [("z", 4, 2), ("z", 5, 2), ("z", 4, 3), ("z", 5, 3), ("s", 6, 3), ("s", 7, 3),
         ("z", 6, 1), ("z", 7, 1), ("y", 4, 0), ("y", 5, 0), ("y", 4, 1), ("y", 5, 1),
         ("y", 4, 2), ("y", 5, 2), ("z", 6, 2), ("z", 7, 2), ("y", 4, 3), ("y", 5, 3)],
    )
    finish(4)
    finish(5)
    tiles(up_tile)

    steps = [(r, far) for r in range(4) for far in (False, True)]

    def index_of(k):
        return owner_of(*steps[k])

    def mine(k):
        return (high == group) if k < per_group else (high != group)

    def slot_of(k):
        return lax.rem(index_of(k), per_group)

    def px_copy(k, which):
        who = 1 - side if which == 0 else side
        return remote(
            to_x.at[k] if k % 2 else outgoing.at[k, who], from_x.at[k, who], px_send.at[k, which], px_recv.at[k, which], beside
        )

    def pz_copy(k):
        i = slot_of(k)
        return remote(to_z.at[i], from_z.at[i], pz_send.at[i], pz_recv.at[i], mate)

    def zz_copy(k):
        s = index_of(k)
        return remote(outgoing.at[k, 1 - side], whole_z.at[s], zz_send.at[s], zz_recv.at[s], mate)

    def down(k):
        r, far = steps[k]
        for array in (6, 7):
            t_copy(array, r, far).wait_recv()
        s = index_of(k)
        weight = down_w[s].reshape(width, block)
        part = jnp.dot(hidden[...], weight, preferred_element_type=jnp.float32)
        part = (part * scales[s, 1:2, :]).astype(jnp.bfloat16)
        outgoing[k, 0] = part[:tokens]
        outgoing[k, 1] = part[tokens:]

        if k % 2:
            zz_copy(k).start()
            return

        @pl.when(jnp.logical_not(mine(k)))
        def _():
            px_copy(k, 0).start()
            px_copy(k, 1).start()

    def pass_on(k):
        if k % 2:
            zz_copy(k).wait_recv()

            @pl.when(jnp.logical_not(mine(k)))
            def _():
                to_x[k] = (
                    outgoing[k, side].astype(jnp.float32) + whole_z[index_of(k)].astype(jnp.float32)
                ).astype(jnp.bfloat16)
                px_copy(k, 1).start()

            return

        @pl.when(mine(k))
        def _():
            px_copy(k, 0).wait_recv()
            to_z[slot_of(k)] = (
                outgoing[k, 1 - side].astype(jnp.float32) + from_x[k, 1 - side].astype(jnp.float32)
            ).astype(jnp.bfloat16)
            pz_copy(k).start()

    def out_copy(k):
        i = slot_of(k)
        target = out_ref.at[:, pl.ds(pl.multiple_of(i * block, block), block)]
        return pltpu.make_async_copy(out_buf.at[i], target, out_sem.at[i])

    def close(k):
        i = slot_of(k)
        s = index_of(k)

        @pl.when(mine(k))
        def _():
            px_copy(k, 1).wait_recv()
            if k % 2 == 0:
                pz_copy(k).wait_recv()
            lines = pl.ds(pl.multiple_of(side * tokens, tokens), tokens)
            total = outgoing[k, side].astype(jnp.float32) + from_x[k, side].astype(jnp.float32)
            total = total + (whole_z[s] if k % 2 else from_z[i]).astype(jnp.float32)
            out_buf[i] = (after[s, lines, :].astype(jnp.float32) + total).astype(jnp.bfloat16)
            out_copy(k).start()

    def take_all(take, r):
        for array in (6, 7):
            take(array, r)

    def early_waits():
        z_copy(0, 3).wait_send()
        z_copy(1, 3).wait_send()

        @pl.when(inner)
        def _():
            for array in range(2, 8):
                for way in (3, 4):
                    z_copy(array, way).wait_send()

        for array in range(8):
            for r in range(4):
                if r in (1, 2):
                    z_copy(array, r).wait_send()
                if array < 6 or r < 3:
                    y_copy(array, r).wait_send()
                    for far in (False, True):
                        t_copy(array, r, far).wait_send()
        for r in range(4):
            for far in (False, True):
                mx_copy(r, far).wait_send()
                mt_copy(r, far).wait_send()
        for copy in scale_copies + mix_copies + [res_z, res_x, res_d]:
            copy.wait_send()

    each([("z", 6, 2), ("z", 7, 2)], [])
    down(0)
    take_all(take_y, 0)
    down(1)
    down(2)
    take_all(take_y, 1)
    down(3)
    down(4)
    take_all(take_z, 3)
    take_all(take_y, 2)
    down(5)
    down(6)
    pass_on(1)
    pass_on(3)
    pass_on(0)
    pass_on(4)
    early_waits()
    take_y(6, 3)
    pass_on(2)
    take_y(7, 3)
    down(7)
    pass_on(5)
    pass_on(6)
    close(0)
    close(2)
    close(4)
    pass_on(7)
    for k in (1, 3, 6, 5, 7):
        close(k)

    for array in (6, 7):
        y_copy(array, 3).wait_send()
        t_copy(array, 3, False).wait_send()
        t_copy(array, 3, True).wait_send()
    for k in range(shards):
        if k % 2:
            zz_copy(k).wait_send()
        else:
            pl.when(mine(k))(pz_copy(k).wait_send)

        @pl.when(jnp.logical_not(mine(k)))
        def _():
            if k % 2 == 0:
                px_copy(k, 0).wait_send()
            px_copy(k, 1).wait_send()

    for k in range(shards):
        pl.when(mine(k))(out_copy(k).wait)


def fused(
    shards, residual, small, raw,
):
    own_width, tokens = residual.shape
    features = 2 * own_width
    short = jnp.bfloat16
    in_rows, mix_width = raw[0].shape
    rows, narrow = in_rows // 2, mix_width // 2
    ff = raw[4].shape[1]
    width = ff // 2
    out_rows, block = raw[3].shape
    channels = 2 * out_rows
    tall = width // 2
    steps = shards
    vmem = pl.BlockSpec(memory_space=pltpu.VMEM)
    dma = pltpu.SemaphoreType.DMA
    return pl.pallas_call(
        functools.partial(layer_kernel, channels, LEN),
        out_shape=jax.ShapeDtypeStruct((tokens, own_width), short),
        in_specs=[vmem] * (1 + len(small)) + [pl.BlockSpec(memory_space=pl.ANY)] * 7,
        out_specs=pl.BlockSpec(memory_space=pl.ANY),
        scratch_shapes=[
            pltpu.VMEM((shards, 2, rows, 3 * narrow), short),
            pltpu.VMEM((shards, 2, 2, out_rows // 2, block), short),
            pltpu.VMEM((shards, 2, 2, rows // 2, width), short),
            pltpu.VMEM((shards, 2, 2, rows // 2, width), short),
            pltpu.VMEM((shards, 2, 2, tall // 2, block), short),
            pltpu.VMEM((rows, 3 * narrow), short),
            pltpu.VMEM((rows // 2, width), short),
            pltpu.VMEM((rows // 2, width), short),
            pltpu.VMEM((rows // 2, width), short),
            pltpu.VMEM((rows // 2, width), short),
            pltpu.VMEM((tall // 2, block), short),
            pltpu.VMEM((tall // 2, block), short),
        ]
        + [pltpu.VMEM((rows, mix_width), jnp.float32)] * 3
        + [
            pltpu.VMEM((out_rows // 2, block), jnp.float32),
            pltpu.VMEM((rows, ff), jnp.float32),
            pltpu.VMEM((rows, ff), jnp.float32),
            pltpu.VMEM((2, tall, block), jnp.float32),
            pltpu.VMEM((tokens, own_width), short),
            pltpu.VMEM((8, block), jnp.float32),
            pltpu.VMEM((2, 2, tokens, own_width), short),
            pltpu.VMEM((shards, 8, block), jnp.float32),
            pltpu.VMEM((2, 8, block), jnp.float32),
            pltpu.VMEM((2, 2, 2 * tokens, narrow), short),
            pltpu.VMEM((shards, 2 * tokens, block), short),
            pltpu.VMEM((2 * tokens, features), short),
            pltpu.VMEM((2 * tokens, width), jnp.float32),
            pltpu.VMEM((2 * tokens, width), short),
            pltpu.VMEM((steps, 2, tokens, block), short),
            pltpu.VMEM((steps, 2, tokens, block), short),
            pltpu.VMEM((steps // 2, tokens, block), short),
            pltpu.VMEM((steps // 2, tokens, block), short),
            pltpu.VMEM((steps, tokens, block), short),
            pltpu.VMEM((steps, tokens, block), short),
            pltpu.VMEM((steps // 2, tokens, block), short),
            dma((8,)),
            dma((8, 4)),
            dma((8, 3)),
            dma((8, 4)),
            dma((8, 4)),
            dma((8, 8)),
            dma((8, 8)),
            dma((8,)),
            dma((8,)),
            dma((8,)),
            dma((8,)),
            dma((3,)),
            dma((3,)),
            dma((shards,)),
            dma((shards,)),
            dma((3,)),
            dma((3,)),
            dma((steps, 2)),
            dma((steps, 2)),
            dma((steps // 2,)),
            dma((steps // 2,)),
            dma((steps,)),
            dma((steps,)),
            dma((steps // 2,)),
        ],
        compiler_params=pltpu.CompilerParams(
            collective_id=1, has_side_effects=True, vmem_limit_bytes=60 * 1024 * 1024
        ),
        name="layer",
    )(
        residual, *small, *raw,
    )


def local(
    reps,
    shards,
    groups,
    residual,
    mixer_gain,
    value_weight,
    value_scale,
    input_gate_weight,
    input_gate_scale,
    output_gate_weight,
    output_gate_scale,
    conv_taps,
    conv_gain,
    mixer_out_weight,
    mixer_out_scale,
    channel_gain,
    gate_weight,
    gate_scale,
    up_weight,
    up_scale,
    down_weight,
    down_scale,
):
    own_rows, tokens = residual.shape
    width = value_weight.shape[1]
    channels = width * groups
    features = own_rows * groups
    short = jnp.bfloat16
    block, ff = mixer_out_weight.shape[1], gate_weight.shape[1]
    in_rows, out_rows = value_weight.shape[0], mixer_out_weight.shape[0]
    if (
        reps == 2 and groups == 2 and shards == 8 and tokens % LEN == 0
        and block % 128 == 0 and width % 256 == 0 and ff % 256 == 0 and block == width
        and in_rows % 64 == 0 and out_rows == width and own_rows == block * shards // 2
    ):
        result = fused(
            shards, residual,
            [mixer_gain[None], value_scale[None], input_gate_scale[None], output_gate_scale[None],
             conv_taps, conv_gain[None], channel_gain[None], gate_scale.reshape(-1, 128),
             up_scale.reshape(-1, 128), mixer_out_scale[None], down_scale[None]],
            [value_weight, input_gate_weight, output_gate_weight, mixer_out_weight,
             gate_weight, up_weight, down_weight],
        )
        return result.T
    projections = jnp.concatenate(
        [value_weight.astype(short), input_gate_weight.astype(short), output_gate_weight.astype(short)],
        axis=1,
    )
    arrays = [
        projections,
        mixer_out_weight.astype(short),
        gate_weight.astype(short),
        up_weight.astype(short),
        down_weight.astype(short),
    ]
    scales = jnp.stack([mixer_out_scale, down_scale])
    (proj_all, out_all, gate_all, up_all, down_all), rows_all, scales_all = gather_all(
        arrays, residual, scales, groups, shards, reps
    )
    whole = rows_all.reshape(features, tokens)
    out_scale = scales_all[:, 0].reshape(features)
    down_scale_full = scales_all[:, 1].reshape(features)

    normed = normalize(whole, mixer_gain)
    projected = contract(proj_all.reshape(features, 3 * width), normed)
    value = projected[:width] * value_scale[:, None]
    in_gate = projected[width : 2 * width] * input_gate_scale[:, None]
    out_gate = projected[2 * width :] * output_gate_scale[:, None]
    mixed = out_gate * causal_conv(in_gate * value, conv_taps, LEN)
    squares = lax.psum(jnp.sum(mixed * mixed, axis=0), "tp")
    conv_normed = (
        mixed * lax.rsqrt(squares / channels + epsilon)[None, :] * conv_gain[:, None]
    ).astype(short)
    part = lax.dot_general(
        out_all, conv_normed, (((1,), (0,)), ((), ())), preferred_element_type=jnp.float32
    ).reshape(features, tokens)
    rounded = (part * out_scale[:, None]).astype(short)
    parts = lax.all_gather(rounded, "tp", axis=0)
    total = jnp.sum(parts.astype(jnp.float32), axis=0)
    after_whole = (whole.astype(jnp.float32) + total).astype(short)
    after_own = lax.dynamic_slice_in_dim(
        after_whole, lax.axis_index("tp") * own_rows, own_rows, 0
    )
    normed_two = normalize(after_whole, channel_gain)
    gate = contract(gate_all.reshape(features, -1), normed_two)
    upper = contract(up_all.reshape(features, -1), normed_two)
    hidden = (jax.nn.silu(gate * gate_scale[:, None]) * (upper * up_scale[:, None])).astype(short)
    down = lax.dot_general(
        down_all, hidden, (((1,), (0,)), ((), ())), preferred_element_type=jnp.float32
    ).reshape(features, tokens)
    total_two = lax.psum_scatter(
        (down * down_scale_full[:, None]).astype(short),
        "tp",
        scatter_dimension=0,
        tiled=True,
    ).astype(jnp.float32)
    return (after_own.astype(jnp.float32) + total_two).astype(short)


def solution(mesh):
    placed = (
        P("tp", ("rep", "fs")),
        P(),
        P("fs", "tp"),
        P("tp"),
        P("fs", "tp"),
        P("tp"),
        P("fs", "tp"),
        P("tp"),
        P(None, "tp"),
        P("tp"),
        P("tp", "fs"),
        P("fs"),
        P(),
        P("fs", "tp"),
        P("tp"),
        P("fs", "tp"),
        P("tp"),
        P("tp", "fs"),
        P("fs"),
    )
    sizes = mesh.shape["rep"], mesh.shape["fs"], mesh.shape["tp"]
    return jax.shard_map(
        functools.partial(local, *sizes),
        mesh=mesh,
        in_specs=placed,
        out_specs=P("tp", ("rep", "fs")),
        check_vma=False,
    )
```

```python
import functools

import jax
import jax.numpy as jnp
from jax import lax
from jax.experimental import pallas as pl
from jax.experimental.pallas import tpu as pltpu
from jax.sharding import PartitionSpec as P

LEN = 128
MESH = pl.DeviceIdType.MESH

epsilon = 1e-06


def contract(weight, rows):
    return lax.dot_general(
        weight, rows, (((0,), (0,)), ((), ())), preferred_element_type=jnp.float32
    )


def normalize(values, gain):
    floats = values.astype(jnp.float32)
    mean = jnp.mean(floats * floats, axis=0, keepdims=True)
    return (floats * lax.rsqrt(mean + epsilon) * gain[:, None]).astype(jnp.bfloat16)


def causal_conv(values, taps, length):
    total = values.shape[1]
    position = jnp.arange(total, dtype=jnp.int32) % length
    shifted_one = jnp.pad(values, ((0, 0), (1, 0)))[:, :total]
    shifted_two = jnp.pad(values, ((0, 0), (2, 0)))[:, :total]
    shifted_one = jnp.where(position[None, :] >= 1, shifted_one, 0.0)
    shifted_two = jnp.where(position[None, :] >= 2, shifted_two, 0.0)
    return (
        taps[2][:, None] * values + taps[1][:, None] * shifted_one + taps[0][:, None] * shifted_two
    )


def ring_plan(sizes, ring):
    free = {"up": 0.0, "down": 0.0, "y": 0.0, "d": 0.0}
    rate = {"up": 46.0, "down": 46.0, "y": 46.0, "d": 330.0}
    waiting = []
    for array in range(len(sizes)):
        for chunk in range(4):
            waiting.append((0.0, array, chunk, 0, 0, None))
    order = []
    pending = []

    def push(ready, send, link, needs):
        pending.append((ready, send, link, needs))

    def ahead(ready, array, chunk, pair, hop, needs):
        link = "up" if chunk % 2 == 0 else "down"
        if hop < ring - 1:
            push(ready, (array, chunk, pair, hop, "z"), link, needs)
        if chunk < 2 and pair == 0 and hop == 0:
            push(ready, (array, chunk, pair, hop, "y"), "y", needs)
        if chunk >= 2 and pair == 0:
            push(ready, (array, chunk, pair, hop, "y"), "y", needs)
        if needs is not None:
            push(ready, (array, chunk, pair, hop, "d"), "d", needs)

    for _, array, chunk, pair, hop, needs in waiting:
        ahead(0.0, array, chunk, pair, hop, needs)
    while pending:
        best = min(
            range(len(pending)),
            key=lambda i: (
                max(pending[i][0], free[pending[i][2]]),
                pending[i][1][0],
                pending[i][0],
                i,
            ),
        )
        ready, send, link, needs = pending.pop(best)
        begin = max(ready, free[link])
        end = begin + sizes[send[0]] / rate[link] / 1e3
        free[link] = end
        order.append((begin, ready, send, needs))
        array, chunk, pair, hop, kind = send
        if kind == "z":
            ahead(end + 2.0, array, chunk, pair, hop + 1, send)
        elif kind == "y":
            if chunk < 2:
                ahead(end + 2.0, array, chunk, 1, 0, send)
            else:
                push(end + 2.0, (array, chunk, 1, hop, "d"), "d", send)
    order.sort(key=lambda item: item[1])
    return [(send, needs) for _, _, send, needs in order]


def gather_kernel(plan, count, groups, shards, *refs):
    own, (own_rows, own_scales) = refs[:count], refs[count : count + 2]
    outs = refs[count + 2 : 2 * count + 2]
    out_rows, out_scales = refs[2 * count + 2 : 2 * count + 4]
    send_sem, recv_sem, local_sem, small_send, small_recv = refs[2 * count + 4 :]
    ring = shards // 2
    place = lax.axis_index("fs")
    core = lax.axis_index("rep")
    group = lax.axis_index("tp")
    z, y = place // 2, place % 2
    up = {"fs": lax.rem(z + 1, ring) * 2 + y}
    down = {"fs": lax.rem(z + ring - 1, ring) * 2 + y}
    across = {"fs": z * 2 + (1 - y)}
    twin = {"rep": 1 - core}

    barrier = pltpu.get_barrier_semaphore()
    others = [{"fs": lax.rem(place + step, shards)} for step in range(1, shards)]
    others += [{"tp": lax.rem(group + step, groups)} for step in range(1, groups)]
    others += [twin]
    for other in others:
        pl.semaphore_signal(barrier, inc=1, device_id=other, device_id_type=MESH)
    pl.semaphore_wait(barrier, len(others))

    small = []
    for step in range(1, groups):
        small.append(
            pltpu.make_async_remote_copy(
                own_rows, out_rows.at[group], small_send.at[step - 1], small_recv.at[step - 1],
                device_id={"tp": lax.rem(group + step, groups)}, device_id_type=MESH,
            )
        )
    for step in range(1, shards):
        index = groups - 1 + step - 1
        small.append(
            pltpu.make_async_remote_copy(
                own_scales, out_scales.at[place], small_send.at[index], small_recv.at[index],
                device_id={"fs": lax.rem(place + step, shards)}, device_id_type=MESH,
            )
        )
    for copy in small:
        copy.start()

    copies = {}
    for number, (send, _) in enumerate(plan):
        array, chunk, pair, hop, kind = send
        step = hop if chunk % 2 == 0 else ring - hop
        owner = lax.rem(z + ring - step, ring) * 2 + (y if pair == 0 else 1 - y)
        slot = outs[array].at[owner, core, chunk]
        source = own[array].at[core, chunk] if (hop == 0 and pair == 0) else slot
        target = {"z": up if chunk % 2 == 0 else down, "y": across, "d": twin}[kind]
        copies[send] = pltpu.make_async_remote_copy(
            source, slot, send_sem.at[number], recv_sem.at[number],
            device_id=target, device_id_type=MESH,
        )

    local = [
        pltpu.make_async_copy(own[array], outs[array].at[place], local_sem.at[array])
        for array in range(count)
    ]
    local.append(pltpu.make_async_copy(own_rows, out_rows.at[group], local_sem.at[count]))
    local.append(pltpu.make_async_copy(own_scales, out_scales.at[place], local_sem.at[count + 1]))

    arrived = set()
    started_local = False
    for send, needs in plan:
        if needs is not None and needs not in arrived:
            if not started_local:
                started_local = True
                for copy in local:
                    copy.start()
            copies[needs].wait_recv()
            arrived.add(needs)
        copies[send].start()
    for send, _ in plan:
        copies[send].wait_send()
        if send not in arrived:
            copies[send].wait_recv()
    for copy in small:
        copy.wait()
    for copy in local:
        copy.wait()


def gather_all(arrays, rows, scales, groups, shards, reps):
    count = len(arrays)
    own = [a.reshape(reps, 4, a.shape[0] // (4 * reps), a.shape[1]) for a in arrays]
    sizes = [a.size // (4 * reps) * a.dtype.itemsize for a in arrays]
    plan = ring_plan(sizes, shards // 2)
    small = groups - 1 + shards - 1
    result = pl.pallas_call(
        functools.partial(gather_kernel, plan, count, groups, shards),
        out_shape=[jax.ShapeDtypeStruct((shards,) + a.shape, a.dtype) for a in own]
        + [
            jax.ShapeDtypeStruct((groups,) + rows.shape, rows.dtype),
            jax.ShapeDtypeStruct((shards,) + scales.shape, scales.dtype),
        ],
        in_specs=[pl.BlockSpec(memory_space=pl.ANY)] * (count + 2),
        out_specs=[pl.BlockSpec(memory_space=pl.ANY)] * (count + 2),
        scratch_shapes=[
            pltpu.SemaphoreType.DMA((len(plan),)),
            pltpu.SemaphoreType.DMA((len(plan),)),
            pltpu.SemaphoreType.DMA((count + 2,)),
            pltpu.SemaphoreType.DMA((small,)),
            pltpu.SemaphoreType.DMA((small,)),
        ],
        compiler_params=pltpu.CompilerParams(collective_id=0, has_side_effects=True),
        name="gather_all",
    )(*own, rows, scales)
    whole = [g.reshape((shards,) + a.shape) for g, a in zip(result, arrays)]
    return whole, result[count], result[count + 1]


def layer_kernel(
    channels, length,
    residual, mixer_gain, value_scale, input_scale, output_scale, taps, conv_gain, channel_gain,
    gate_scale, up_scale, out_scale, down_scale,
    *refs,
):
    raw, out_ref, refs = refs[:7], refs[7], refs[8:]
    bufs, refs = refs[:5], refs[5:]
    others, refs = refs[:7], refs[7:]
    stages, refs = refs[:7], refs[7:]
    (own_res, own_scales, res, scales, gains, mixes, after, normed, gate_buf, hidden, outgoing, from_x, to_z, from_z, to_x, whole_z, out_buf,
     raw_sem, z_send, z_recv, y_send, y_recv, t_send, t_recv, mx_send, mx_recv, mt_send, mt_recv,
     r_send, r_recv, s_send, s_recv, m_send, m_recv, px_send, px_recv, pz_send, pz_recv,
     zz_send, zz_recv, out_sem) = refs
    proj_buf, mout_buf, gate_w, up_w, down_w = bufs
    shards = gate_w.shape[0]
    place = lax.axis_index("fs")
    core = lax.axis_index("rep")
    group = lax.axis_index("tp")
    own_width, tokens = residual.shape
    mix_scales = (value_scale, input_scale, output_scale)
    features = 2 * own_width
    block = mout_buf.shape[-1]
    per_group = shards // 2
    depth = shards // 2
    width = gate_w.shape[-1]
    narrow = mixes.shape[-1]
    all_tokens = 2 * tokens

    z, y = place // 2, place % 2
    side = z % 2
    part_of = ((z + 1) // 2) % 2
    high = (z * 2 + y) // per_group
    pair = z + 1 - 2 * side
    inner = part_of == 1
    outer = part_of == 0
    opposite = 1 - z // 2
    levels = [z, pair, 1 + opposite, (depth - 1) * opposite]
    twin = {"rep": 1 - core}
    across = {"fs": z * 2 + 1 - y}
    beside = {"tp": 1 - group}
    mate = {"fs": pair * 2 + y}
    corner = {"fs": pair * 2 + y, "tp": 1 - group}

    def remote(source, target, send, recv, device):
        return pltpu.make_async_remote_copy(
            source, target, send, recv, device_id=device, device_id_type=MESH
        )

    def spot(array, owner, half):
        if array == 1:
            return mout_buf.at[owner, group, half]
        if array >= 2:
            return bufs[1 + array // 2].at[owner, half, array % 2]
        return proj_buf.at[owner, half]

    def owner_of(r, far):
        return levels[r] * 2 + (1 - y if far else y)

    def z_copy(array, way):
        target = spot(array, pair * 2 + y if way == 4 else place, core)
        if array == 1 or way in (2, 4):
            source = target
        else:
            source = others[array - 1 if array else 0]
        level = (None, pair, depth - 1 - z, depth - 1 - pair, depth - 1 - z)[way]
        kind = (None, 0, 2 - part_of, 2 - part_of, 2)[way]
        return remote(
            source, target, z_send.at[array, way - 1], z_recv.at[array, kind],
            {"fs": level * 2 + y},
        )

    def z_wait(array, r):
        target = spot(array, owner_of(r, False), core)
        remote(
            target, target, z_send.at[array, r - 1], z_recv.at[array, r - 1], across
        ).wait_recv()

    def y_copy(array, r):
        target = spot(array, owner_of(r, False), core)
        return remote(target, target, y_send.at[array, r], y_recv.at[array, r], across)

    def t_copy(array, r, far):
        target = spot(array, owner_of(r, far), core)
        index = r + 4 * far
        return remote(target, target, t_send.at[array, index], t_recv.at[array, index], twin)

    def mx_copy(r, far):
        target = spot(1, owner_of(r, far), core)
        index = r + 4 * far
        return remote(target, target, mx_send.at[index], mx_recv.at[index], beside)

    def mt_copy(r, far):
        target = mout_buf.at[owner_of(r, far), 1 - group, core]
        index = r + 4 * far
        return remote(target, target, mt_send.at[index], mt_recv.at[index], twin)

    rows = stages[0].shape[0]
    tall = stages[6].shape[1]
    raw_copies = []
    for i in range(4):
        raw_copies.append([pltpu.make_async_copy(
            raw[i].at[pl.ds(pl.multiple_of(core * rows, rows), rows)], stages[i], raw_sem.at[i])])
    for i in range(4, 6):
        raw_copies.append([pltpu.make_async_copy(
            raw[i].at[pl.ds(pl.multiple_of(core * rows, rows), rows)], stages[i], raw_sem.at[i])])
    raw_copies.append([
        pltpu.make_async_copy(
            raw[6].at[pl.ds(pl.multiple_of(k * width + core * tall, 16), tall)],
            stages[6].at[k], raw_sem.at[6 + k])
        for k in range(2)
    ])
    for group_of in raw_copies:
        for copy in group_of:
            copy.start()

    for first in range(0, own_width, tokens):
        own_res[:, first : first + tokens] = residual[first : first + tokens, :].T
    own_scales[...] = jnp.concatenate(
        [out_scale[...], down_scale[...], conv_gain[...], jnp.zeros((5, block), jnp.float32)], axis=0
    )

    barrier = pltpu.get_barrier_semaphore()
    partners = [{"fs": lax.rem(place + step, shards)} for step in range(1, shards)]
    partners += [beside, corner, twin]
    for other in partners:
        pl.semaphore_signal(barrier, inc=1, device_id=other, device_id_type=MESH)
    pl.semaphore_wait(barrier, len(partners))

    scale_copies = [
        remote(own_scales, scales.at[place], s_send.at[step], s_recv.at[step],
               {"fs": lax.rem(place + step, shards)})
        for step in range(1, shards)
    ]
    scale_copies.append(remote(own_scales, gains.at[group], s_send.at[0], s_recv.at[0], beside))
    res_z = remote(own_res, res.at[side, group], r_send.at[0], r_recv.at[0], mate)
    res_x = remote(own_res, res.at[side, group], r_send.at[1], r_recv.at[1], beside)
    passed = res.at[1 - side, group]
    res_d = remote(passed, passed, r_send.at[2], r_recv.at[2], beside)

    def start_z(*pairs):
        for array, r in pairs:
            z_copy(array, r).start()

    def start_inner(*pairs):
        @pl.when(inner)
        def _():
            for array, way in pairs:
                z_copy(array, way).start()

    def start_outer(*pairs):
        @pl.when(outer)
        def _():
            for array, way in pairs:
                z_copy(array, way).start()

    def wait_raw(*indices):
        for i in indices:
            for copy in raw_copies[i]:
                copy.wait()

    def both(first, second, size):
        return [
            (first, pl.ds(pl.multiple_of(part_of * size, 128), size)),
            (second, pl.ds(pl.multiple_of((1 - part_of) * size, 128), size)),
        ]

    res_z.start()
    res_x.start()
    wait_raw(0, 1, 2)
    for i in range(3):
        for target, cols in both(proj_buf.at[place, core], others[0], narrow):
            target[:, i * narrow : (i + 1) * narrow] = stages[i][:, cols].astype(jnp.bfloat16)
    start_z((0, 1), (0, 2), (0, 3))
    y_copy(0, 0).start()
    t_copy(0, 0, False).start()
    wait_raw(3)
    mout_buf[place, group, core] = stages[3][...].astype(jnp.bfloat16)
    start_z((1, 1), (1, 2), (1, 3))
    y_copy(1, 0).start()
    mx_copy(0, False).start()
    t_copy(1, 0, False).start()
    for copy in scale_copies:
        copy.start()
    fine = rows // 2
    for matrix in (1, 2):
        wait_raw(matrix + 3)
        for chunk in range(2):
            array = 2 * matrix + chunk
            lines = slice(chunk * fine, (chunk + 1) * fine)
            for target, cols in both(spot(array, place, core), others[array - 1], width):
                target[...] = stages[matrix + 3][lines, cols].astype(jnp.bfloat16)
            t_copy(array, 0, False).start()
            if matrix == 1:
                y_copy(array, 0).start()
                if chunk == 0:
                    start_z((array, 1))
                else:
                    start_outer((array, 1))
                start_inner((array, 2))
    wait_raw(6)
    short = tall // 2
    for chunk in range(2):
        array = 6 + chunk
        lines = slice(chunk * short, (chunk + 1) * short)
        down_w[place, core, chunk] = stages[6][part_of, lines, :].astype(jnp.bfloat16)
        others[array - 1][...] = stages[6][1 - part_of, lines, :].astype(jnp.bfloat16)
        t_copy(array, 0, False).start()
    res[side, group] = own_res[...]
    scales[place] = own_scales[...]
    gains[group] = own_scales[...]

    def take_z(array, r):
        z_wait(array, r)
        if r == 1 and array >= 2:
            start_inner((array, 4))
        y_copy(array, r).start()
        t_copy(array, r, False).start()
        if array == 1:
            mx_copy(r, False).start()

    def take_y(array, r):
        y_copy(array, r).wait_recv()
        t_copy(array, r, True).start()
        if array == 1:
            mx_copy(r, True).start()

    def run(items):
        for kind, array, r in items:
            if kind == "s":
                z_copy(array, r).start()
            elif kind == "o":
                y_copy(array, r).start()
            else:
                (take_z if kind == "z" else take_y)(array, r)

    def each(outer_items, inner_items):
        @pl.when(outer)
        def _():
            run(outer_items)

        @pl.when(inner)
        def _():
            run(inner_items)

    def finish(array):
        for far in (False, True):
            for r in range(4):
                t_copy(array, r, far).wait_recv()

    def scaled(squares, count):
        return lax.rsqrt(squares / count + epsilon)

    def normalize_side(s):
        floats = [res[s, k].astype(jnp.float32) for k in range(2)]
        squares = sum(jnp.sum(row * row, axis=1, keepdims=True) for row in floats)
        factor = scaled(squares, features)
        lines = pl.ds(pl.multiple_of(s * tokens, tokens), tokens)
        for k in range(2):
            cols = slice(k * own_width, (k + 1) * own_width)
            normed[lines, cols] = (
                res[s, k].astype(jnp.float32) * factor * mixer_gain[:, cols]
            ).astype(jnp.bfloat16)

    order = (1, 2, 3)
    take_z(0, 2)
    take_z(1, 2)
    for array in (4, 5):
        y_copy(array, 0).start()
    res_z.wait_recv()
    res_d.start()
    start_inner((2, 3), (3, 3))
    start_outer((2, 2), (3, 2))
    take_z(0, 1)
    take_z(0, 3)
    for array in (6, 7):
        y_copy(array, 0).start()
    res_x.wait_recv()
    normalize_side(side)
    for r in (0, 2, 1, 3):
        take_y(0, r)
    res_d.wait_recv()
    normalize_side(1 - side)
    finish(0)

    own_cols = pl.ds(pl.multiple_of(part_of * narrow, 128), narrow)

    def project(index):
        weight = proj_buf[:, :, :, index * narrow : (index + 1) * narrow].reshape(features, narrow)
        product = jnp.dot(normed[...], weight, preferred_element_type=jnp.float32)
        return product * mix_scales[index][:, own_cols]

    value = project(0)
    u = project(1) * value
    place_in = lax.rem(lax.broadcasted_iota(jnp.int32, u.shape, 0), length)
    one = jnp.where(place_in >= 1, pltpu.roll(u, 1, 0), 0.0)
    two = jnp.where(place_in >= 2, pltpu.roll(u, 2, 0), 0.0)
    conv = taps[2:3, own_cols] * u + taps[1:2, own_cols] * one + taps[0:1, own_cols] * two
    mixes[group, part_of] = (project(2) * conv).astype(jnp.bfloat16)
    mix_slot = mixes.at[group, part_of]
    mix_copies = [
        remote(mix_slot, mix_slot, m_send.at[i], m_recv.at[i], device)
        for i, device in enumerate((mate, beside, corner))
    ]
    for copy in mix_copies:
        copy.start()
    start_inner((3, 1))
    start_z((4, 1), (5, 1))
    start_outer((4, 2), (5, 2))
    start_z((6, 1), (7, 1))
    each(
        [("z", 1, 3), ("z", 2, 2), ("z", 2, 3), ("z", 1, 1), ("z", 3, 2), ("z", 3, 3)],
        [("z", 1, 1), ("z", 1, 3), ("z", 2, 2), ("z", 3, 2), ("z", 2, 1), ("z", 3, 1),
         ("s", 4, 2), ("s", 4, 3), ("s", 5, 2), ("s", 5, 3)],
    )
    for r in (0, 2, 1, 3):
        take_y(1, r)
    for far in (False, True):
        for r in range(4):
            mx_copy(r, far).wait_recv()
            mt_copy(r, far).start()
    each([("z", 2, 1)], [])
    for copy in scale_copies + mix_copies:
        copy.wait_recv()
    finish(1)
    for far in (False, True):
        for r in range(4):
            mt_copy(r, far).wait_recv()
    total = jnp.zeros((all_tokens, 1), jnp.float32)
    for k in range(2):
        for b in range(2):
            lines = mixes[k, b].astype(jnp.float32)
            total = total + jnp.sum(lines * lines, axis=1, keepdims=True)
    factor = scaled(total, channels)
    for k in range(2):
        for b in range(2):
            cols = slice((2 * k + b) * narrow, (2 * k + b + 1) * narrow)
            hidden[:, cols] = (
                mixes[k, b].astype(jnp.float32) * factor
                * gains[k, 2:3, b * narrow : (b + 1) * narrow]
            ).astype(jnp.bfloat16)
    squares = jnp.zeros((all_tokens, 1), jnp.float32)
    for s in range(shards):
        k, inside = s // per_group, (s % per_group) * block
        part = jnp.dot(
            hidden[:, : 4 * narrow], mout_buf[s].reshape(4 * narrow, block),
            preferred_element_type=jnp.float32,
        ) * scales[s, 0:1, :]
        base = res[:, k, :, inside : inside + block].reshape(all_tokens, block)
        row = (base.astype(jnp.float32) + part).astype(jnp.bfloat16)
        after[s] = row
        row = row.astype(jnp.float32)
        squares = squares + jnp.sum(row * row, axis=1, keepdims=True)
    factor = scaled(squares, features)
    for s in range(shards):
        cols = slice(s * block, (s + 1) * block)
        normed[:, cols] = (
            after[s].astype(jnp.float32) * factor * channel_gain[:, cols]
        ).astype(jnp.bfloat16)

    def tiles(body):
        tile = 256
        whole = width // tile

        @pl.loop(0, whole)
        def _(j):
            body(pl.multiple_of(j * tile, tile), tile)

        if width % tile:
            body(whole * tile, width % tile)

    def multiply(weights, start, size):
        weight = weights[:, :, :, :, pl.ds(start, size)].reshape(features, size)
        return jnp.dot(normed[...], weight, preferred_element_type=jnp.float32)

    def scale_at(scale, start, size):
        first = part_of * (width // 128) + start // 128
        lines = [scale[pl.ds(first + i, 1), :] for i in range(size // 128)]
        return jnp.concatenate(lines, axis=1)

    def gate_tile(start, size):
        gate_buf[:, pl.ds(start, size)] = multiply(gate_w, start, size) * scale_at(
            gate_scale, start, size
        )

    def up_tile(start, size):
        product = multiply(up_w, start, size) * scale_at(up_scale, start, size)
        gate = gate_buf[:, pl.ds(start, size)]
        hidden[:, pl.ds(start, size)] = (
            gate / (1.0 + jnp.exp(-gate)) * product
        ).astype(jnp.bfloat16)

    each(
        [("z", 4, 2), ("z", 4, 3), ("z", 3, 1), ("z", 5, 2), ("z", 5, 3)],
        [("z", 2, 3), ("z", 3, 3), ("z", 4, 1), ("z", 5, 1), ("s", 6, 2), ("s", 7, 2)],
    )
    for array in (2, 3):
        for r in (0,) + order:
            take_y(array, r)
    finish(2)
    finish(3)
    tiles(gate_tile)
    each(
        [("s", 6, 2), ("s", 7, 2),
         ("z", 4, 1), ("z", 5, 1), ("z", 6, 1), ("z", 7, 1),
         ("y", 4, 0), ("y", 5, 0), ("y", 4, 2), ("y", 4, 3), ("y", 5, 2), ("y", 5, 3),
         ("y", 4, 1), ("y", 5, 1)],
        [("z", 4, 2), ("z", 5, 2), ("z", 4, 3), ("z", 5, 3), ("s", 6, 3), ("s", 7, 3),
         ("z", 6, 1), ("z", 7, 1), ("y", 4, 0), ("y", 5, 0), ("y", 4, 1), ("y", 5, 1),
         ("y", 4, 2), ("y", 5, 2), ("z", 6, 2), ("z", 7, 2), ("y", 4, 3), ("y", 5, 3)],
    )
    finish(4)
    finish(5)
    tiles(up_tile)

    steps = [(r, far) for r in range(4) for far in (False, True)]

    def index_of(k):
        return owner_of(*steps[k])

    def mine(k):
        return (high == group) if k < per_group else (high != group)

    def slot_of(k):
        return lax.rem(index_of(k), per_group)

    last = shards - 1
    strip = tokens // 2

    def px_copy(k, which):
        sems = px_send.at[k, which], px_recv.at[k, which], beside
        if k == last:
            lines = pl.ds(which * strip, strip)
            return remote(to_x.at[k, lines], from_x.at[k, side, lines], *sems)
        who = 1 - side if which == 0 else side
        source = to_x.at[k] if k % 2 else outgoing.at[k, who]
        return remote(source, from_x.at[k, who], *sems)

    def pz_copy(k):
        i = slot_of(k)
        return remote(to_z.at[i], from_z.at[i], pz_send.at[i], pz_recv.at[i], mate)

    def zz_copies(k):
        s = index_of(k)
        mates = outgoing.at[k, 1 - side]
        if k < last:
            return [remote(mates, whole_z.at[s], zz_send.at[s], zz_recv.at[s], mate)]
        copies = []
        for half, index in ((0, s), (1, shards)):
            lines = pl.ds(half * strip, strip)
            copies.append(remote(
                outgoing.at[k, 1 - side, lines], whole_z.at[s, lines],
                zz_send.at[index], zz_recv.at[index], mate,
            ))
        return copies

    def down(k):
        r, far = steps[k]
        for array in (6, 7):
            t_copy(array, r, far).wait_recv()
        s = index_of(k)
        weight = down_w[s].reshape(width, block)
        part = jnp.dot(hidden[...], weight, preferred_element_type=jnp.float32)
        part = (part * scales[s, 1:2, :]).astype(jnp.bfloat16)
        outgoing[k, 0] = part[:tokens]
        outgoing[k, 1] = part[tokens:]

        if k % 2:
            for copy in zz_copies(k):
                copy.start()
            return

        @pl.when(jnp.logical_not(mine(k)))
        def _():
            px_copy(k, 0).start()
            px_copy(k, 1).start()

    def pass_on(k):
        if k % 2:
            copies = zz_copies(k)
            for which, copy in enumerate(copies):
                copy.wait_recv()
                size = tokens // len(copies)
                lines = slice(which * size, (which + 1) * size)

                @pl.when(jnp.logical_not(mine(k)))
                def _():
                    to_x[k, lines] = (
                        outgoing[k, side, lines].astype(jnp.float32)
                        + whole_z[index_of(k), lines].astype(jnp.float32)
                    ).astype(jnp.bfloat16)
                    px_copy(k, which if k == last else 1).start()

            return

        @pl.when(mine(k))
        def _():
            px_copy(k, 0).wait_recv()
            to_z[slot_of(k)] = (
                outgoing[k, 1 - side].astype(jnp.float32) + from_x[k, 1 - side].astype(jnp.float32)
            ).astype(jnp.bfloat16)
            pz_copy(k).start()

    def out_copy(k):
        i = slot_of(k)
        target = out_ref.at[:, pl.ds(pl.multiple_of(i * block, block), block)]
        return pltpu.make_async_copy(out_buf.at[i], target, out_sem.at[i])

    def close(k):
        i = slot_of(k)
        s = index_of(k)

        @pl.when(mine(k))
        def _():
            px_copy(k, 1).wait_recv()
            if k == last:
                px_copy(k, 0).wait_recv()
            if k % 2 == 0:
                pz_copy(k).wait_recv()
            lines = pl.ds(pl.multiple_of(side * tokens, tokens), tokens)
            total = outgoing[k, side].astype(jnp.float32) + from_x[k, side].astype(jnp.float32)
            total = total + (whole_z[s] if k % 2 else from_z[i]).astype(jnp.float32)
            out_buf[i] = (after[s, lines, :].astype(jnp.float32) + total).astype(jnp.bfloat16)
            out_copy(k).start()

    def take_all(take, r):
        for array in (6, 7):
            take(array, r)

    def early_waits():
        z_copy(0, 3).wait_send()
        z_copy(1, 3).wait_send()

        @pl.when(inner)
        def _():
            for array in range(2, 8):
                for way in (3, 4):
                    z_copy(array, way).wait_send()

        for array in range(8):
            for r in range(4):
                if r in (1, 2):
                    z_copy(array, r).wait_send()
                if array < 6 or r < 3:
                    y_copy(array, r).wait_send()
                    for far in (False, True):
                        t_copy(array, r, far).wait_send()
        for r in range(4):
            for far in (False, True):
                mx_copy(r, far).wait_send()
                mt_copy(r, far).wait_send()
        for copy in scale_copies + mix_copies + [res_z, res_x, res_d]:
            copy.wait_send()

    each([("z", 6, 2), ("z", 7, 2)], [])
    down(0)
    take_all(take_y, 0)
    down(1)
    down(2)
    take_all(take_y, 1)
    each([("z", 6, 3), ("z", 7, 3)], [])
    down(3)
    down(4)
    each([], [("z", 6, 3), ("z", 7, 3)])
    take_all(take_y, 2)
    down(5)
    down(6)
    pass_on(1)
    pass_on(3)
    pass_on(0)
    pass_on(4)
    early_waits()
    take_y(6, 3)
    pass_on(2)
    take_y(7, 3)
    down(7)
    pass_on(5)
    pass_on(6)
    close(0)
    close(2)
    close(4)
    pass_on(7)
    for k in (1, 3, 6, 5, 7):
        close(k)

    for array in (6, 7):
        y_copy(array, 3).wait_send()
        t_copy(array, 3, False).wait_send()
        t_copy(array, 3, True).wait_send()
    for k in range(shards):
        if k % 2:
            for copy in zz_copies(k):
                copy.wait_send()
        else:
            pl.when(mine(k))(pz_copy(k).wait_send)

        @pl.when(jnp.logical_not(mine(k)))
        def _():
            if k % 2 == 0 or k == last:
                px_copy(k, 0).wait_send()
            px_copy(k, 1).wait_send()

    for k in range(shards):
        pl.when(mine(k))(out_copy(k).wait)


def fused(
    shards, residual, small, raw,
):
    own_width, tokens = residual.shape
    features = 2 * own_width
    short = jnp.bfloat16
    in_rows, mix_width = raw[0].shape
    rows, narrow = in_rows // 2, mix_width // 2
    ff = raw[4].shape[1]
    width = ff // 2
    out_rows, block = raw[3].shape
    channels = 2 * out_rows
    tall = width // 2
    steps = shards
    vmem = pl.BlockSpec(memory_space=pltpu.VMEM)
    dma = pltpu.SemaphoreType.DMA
    return pl.pallas_call(
        functools.partial(layer_kernel, channels, LEN),
        out_shape=jax.ShapeDtypeStruct((tokens, own_width), short),
        in_specs=[vmem] * (1 + len(small)) + [pl.BlockSpec(memory_space=pl.ANY)] * 7,
        out_specs=pl.BlockSpec(memory_space=pl.ANY),
        scratch_shapes=[
            pltpu.VMEM((shards, 2, rows, 3 * narrow), short),
            pltpu.VMEM((shards, 2, 2, out_rows // 2, block), short),
            pltpu.VMEM((shards, 2, 2, rows // 2, width), short),
            pltpu.VMEM((shards, 2, 2, rows // 2, width), short),
            pltpu.VMEM((shards, 2, 2, tall // 2, block), short),
            pltpu.VMEM((rows, 3 * narrow), short),
            pltpu.VMEM((rows // 2, width), short),
            pltpu.VMEM((rows // 2, width), short),
            pltpu.VMEM((rows // 2, width), short),
            pltpu.VMEM((rows // 2, width), short),
            pltpu.VMEM((tall // 2, block), short),
            pltpu.VMEM((tall // 2, block), short),
        ]
        + [pltpu.VMEM((rows, mix_width), jnp.float32)] * 3
        + [
            pltpu.VMEM((out_rows // 2, block), jnp.float32),
            pltpu.VMEM((rows, ff), jnp.float32),
            pltpu.VMEM((rows, ff), jnp.float32),
            pltpu.VMEM((2, tall, block), jnp.float32),
            pltpu.VMEM((tokens, own_width), short),
            pltpu.VMEM((8, block), jnp.float32),
            pltpu.VMEM((2, 2, tokens, own_width), short),
            pltpu.VMEM((shards, 8, block), jnp.float32),
            pltpu.VMEM((2, 8, block), jnp.float32),
            pltpu.VMEM((2, 2, 2 * tokens, narrow), short),
            pltpu.VMEM((shards, 2 * tokens, block), short),
            pltpu.VMEM((2 * tokens, features), short),
            pltpu.VMEM((2 * tokens, width), jnp.float32),
            pltpu.VMEM((2 * tokens, width), short),
            pltpu.VMEM((steps, 2, tokens, block), short),
            pltpu.VMEM((steps, 2, tokens, block), short),
            pltpu.VMEM((steps // 2, tokens, block), short),
            pltpu.VMEM((steps // 2, tokens, block), short),
            pltpu.VMEM((steps, tokens, block), short),
            pltpu.VMEM((steps, tokens, block), short),
            pltpu.VMEM((steps // 2, tokens, block), short),
            dma((8,)),
            dma((8, 4)),
            dma((8, 3)),
            dma((8, 4)),
            dma((8, 4)),
            dma((8, 8)),
            dma((8, 8)),
            dma((8,)),
            dma((8,)),
            dma((8,)),
            dma((8,)),
            dma((3,)),
            dma((3,)),
            dma((shards,)),
            dma((shards,)),
            dma((3,)),
            dma((3,)),
            dma((steps, 2)),
            dma((steps, 2)),
            dma((steps // 2,)),
            dma((steps // 2,)),
            dma((steps + 1,)),
            dma((steps + 1,)),
            dma((steps // 2,)),
        ],
        compiler_params=pltpu.CompilerParams(
            collective_id=1, has_side_effects=True, vmem_limit_bytes=60 * 1024 * 1024
        ),
        name="layer",
    )(
        residual, *small, *raw,
    )


def local(
    reps,
    shards,
    groups,
    residual,
    mixer_gain,
    value_weight,
    value_scale,
    input_gate_weight,
    input_gate_scale,
    output_gate_weight,
    output_gate_scale,
    conv_taps,
    conv_gain,
    mixer_out_weight,
    mixer_out_scale,
    channel_gain,
    gate_weight,
    gate_scale,
    up_weight,
    up_scale,
    down_weight,
    down_scale,
):
    own_rows, tokens = residual.shape
    width = value_weight.shape[1]
    channels = width * groups
    features = own_rows * groups
    short = jnp.bfloat16
    block, ff = mixer_out_weight.shape[1], gate_weight.shape[1]
    in_rows, out_rows = value_weight.shape[0], mixer_out_weight.shape[0]
    if (
        reps == 2 and groups == 2 and shards == 8 and tokens % LEN == 0
        and block % 128 == 0 and width % 256 == 0 and ff % 256 == 0 and block == width
        and in_rows % 64 == 0 and out_rows == width and own_rows == block * shards // 2
    ):
        result = fused(
            shards, residual,
            [mixer_gain[None], value_scale[None], input_gate_scale[None], output_gate_scale[None],
             conv_taps, conv_gain[None], channel_gain[None], gate_scale.reshape(-1, 128),
             up_scale.reshape(-1, 128), mixer_out_scale[None], down_scale[None]],
            [value_weight, input_gate_weight, output_gate_weight, mixer_out_weight,
             gate_weight, up_weight, down_weight],
        )
        return result.T
    projections = jnp.concatenate(
        [value_weight.astype(short), input_gate_weight.astype(short), output_gate_weight.astype(short)],
        axis=1,
    )
    arrays = [
        projections,
        mixer_out_weight.astype(short),
        gate_weight.astype(short),
        up_weight.astype(short),
        down_weight.astype(short),
    ]
    scales = jnp.stack([mixer_out_scale, down_scale])
    (proj_all, out_all, gate_all, up_all, down_all), rows_all, scales_all = gather_all(
        arrays, residual, scales, groups, shards, reps
    )
    whole = rows_all.reshape(features, tokens)
    out_scale = scales_all[:, 0].reshape(features)
    down_scale_full = scales_all[:, 1].reshape(features)

    normed = normalize(whole, mixer_gain)
    projected = contract(proj_all.reshape(features, 3 * width), normed)
    value = projected[:width] * value_scale[:, None]
    in_gate = projected[width : 2 * width] * input_gate_scale[:, None]
    out_gate = projected[2 * width :] * output_gate_scale[:, None]
    mixed = out_gate * causal_conv(in_gate * value, conv_taps, LEN)
    squares = lax.psum(jnp.sum(mixed * mixed, axis=0), "tp")
    conv_normed = (
        mixed * lax.rsqrt(squares / channels + epsilon)[None, :] * conv_gain[:, None]
    ).astype(short)
    part = lax.dot_general(
        out_all, conv_normed, (((1,), (0,)), ((), ())), preferred_element_type=jnp.float32
    ).reshape(features, tokens)
    rounded = (part * out_scale[:, None]).astype(short)
    parts = lax.all_gather(rounded, "tp", axis=0)
    total = jnp.sum(parts.astype(jnp.float32), axis=0)
    after_whole = (whole.astype(jnp.float32) + total).astype(short)
    after_own = lax.dynamic_slice_in_dim(
        after_whole, lax.axis_index("tp") * own_rows, own_rows, 0
    )
    normed_two = normalize(after_whole, channel_gain)
    gate = contract(gate_all.reshape(features, -1), normed_two)
    upper = contract(up_all.reshape(features, -1), normed_two)
    hidden = (jax.nn.silu(gate * gate_scale[:, None]) * (upper * up_scale[:, None])).astype(short)
    down = lax.dot_general(
        down_all, hidden, (((1,), (0,)), ((), ())), preferred_element_type=jnp.float32
    ).reshape(features, tokens)
    total_two = lax.psum_scatter(
        (down * down_scale_full[:, None]).astype(short),
        "tp",
        scatter_dimension=0,
        tiled=True,
    ).astype(jnp.float32)
    return (after_own.astype(jnp.float32) + total_two).astype(short)


def solution(mesh):
    placed = (
        P("tp", ("rep", "fs")),
        P(),
        P("fs", "tp"),
        P("tp"),
        P("fs", "tp"),
        P("tp"),
        P("fs", "tp"),
        P("tp"),
        P(None, "tp"),
        P("tp"),
        P("tp", "fs"),
        P("fs"),
        P(),
        P("fs", "tp"),
        P("tp"),
        P("fs", "tp"),
        P("tp"),
        P("tp", "fs"),
        P("fs"),
    )
    sizes = mesh.shape["rep"], mesh.shape["fs"], mesh.shape["tp"]
    return jax.shard_map(
        functools.partial(local, *sizes),
        mesh=mesh,
        in_specs=placed,
        out_specs=P("tp", ("rep", "fs")),
        check_vma=False,
    )
```

```python
import functools

import jax
import jax.numpy as jnp
from jax import lax
from jax.experimental import pallas as pl
from jax.experimental.pallas import tpu as pltpu
from jax.sharding import PartitionSpec as P

LEN = 128
MESH = pl.DeviceIdType.MESH

epsilon = 1e-06


def contract(weight, rows):
    return lax.dot_general(
        weight, rows, (((0,), (0,)), ((), ())), preferred_element_type=jnp.float32
    )


def normalize(values, gain):
    floats = values.astype(jnp.float32)
    mean = jnp.mean(floats * floats, axis=0, keepdims=True)
    return (floats * lax.rsqrt(mean + epsilon) * gain[:, None]).astype(jnp.bfloat16)


def causal_conv(values, taps, length):
    total = values.shape[1]
    position = jnp.arange(total, dtype=jnp.int32) % length
    shifted_one = jnp.pad(values, ((0, 0), (1, 0)))[:, :total]
    shifted_two = jnp.pad(values, ((0, 0), (2, 0)))[:, :total]
    shifted_one = jnp.where(position[None, :] >= 1, shifted_one, 0.0)
    shifted_two = jnp.where(position[None, :] >= 2, shifted_two, 0.0)
    return (
        taps[2][:, None] * values + taps[1][:, None] * shifted_one + taps[0][:, None] * shifted_two
    )


def ring_plan(sizes, ring):
    free = {"up": 0.0, "down": 0.0, "y": 0.0, "d": 0.0}
    rate = {"up": 46.0, "down": 46.0, "y": 46.0, "d": 330.0}
    waiting = []
    for array in range(len(sizes)):
        for chunk in range(4):
            waiting.append((0.0, array, chunk, 0, 0, None))
    order = []
    pending = []

    def push(ready, send, link, needs):
        pending.append((ready, send, link, needs))

    def ahead(ready, array, chunk, pair, hop, needs):
        link = "up" if chunk % 2 == 0 else "down"
        if hop < ring - 1:
            push(ready, (array, chunk, pair, hop, "z"), link, needs)
        if chunk < 2 and pair == 0 and hop == 0:
            push(ready, (array, chunk, pair, hop, "y"), "y", needs)
        if chunk >= 2 and pair == 0:
            push(ready, (array, chunk, pair, hop, "y"), "y", needs)
        if needs is not None:
            push(ready, (array, chunk, pair, hop, "d"), "d", needs)

    for _, array, chunk, pair, hop, needs in waiting:
        ahead(0.0, array, chunk, pair, hop, needs)
    while pending:
        best = min(
            range(len(pending)),
            key=lambda i: (
                max(pending[i][0], free[pending[i][2]]),
                pending[i][1][0],
                pending[i][0],
                i,
            ),
        )
        ready, send, link, needs = pending.pop(best)
        begin = max(ready, free[link])
        end = begin + sizes[send[0]] / rate[link] / 1e3
        free[link] = end
        order.append((begin, ready, send, needs))
        array, chunk, pair, hop, kind = send
        if kind == "z":
            ahead(end + 2.0, array, chunk, pair, hop + 1, send)
        elif kind == "y":
            if chunk < 2:
                ahead(end + 2.0, array, chunk, 1, 0, send)
            else:
                push(end + 2.0, (array, chunk, 1, hop, "d"), "d", send)
    order.sort(key=lambda item: item[1])
    return [(send, needs) for _, _, send, needs in order]


def gather_kernel(plan, count, groups, shards, *refs):
    own, (own_rows, own_scales) = refs[:count], refs[count : count + 2]
    outs = refs[count + 2 : 2 * count + 2]
    out_rows, out_scales = refs[2 * count + 2 : 2 * count + 4]
    send_sem, recv_sem, local_sem, small_send, small_recv = refs[2 * count + 4 :]
    ring = shards // 2
    place = lax.axis_index("fs")
    core = lax.axis_index("rep")
    group = lax.axis_index("tp")
    z, y = place // 2, place % 2
    up = {"fs": lax.rem(z + 1, ring) * 2 + y}
    down = {"fs": lax.rem(z + ring - 1, ring) * 2 + y}
    across = {"fs": z * 2 + (1 - y)}
    twin = {"rep": 1 - core}

    barrier = pltpu.get_barrier_semaphore()
    others = [{"fs": lax.rem(place + step, shards)} for step in range(1, shards)]
    others += [{"tp": lax.rem(group + step, groups)} for step in range(1, groups)]
    others += [twin]
    for other in others:
        pl.semaphore_signal(barrier, inc=1, device_id=other, device_id_type=MESH)
    pl.semaphore_wait(barrier, len(others))

    small = []
    for step in range(1, groups):
        small.append(
            pltpu.make_async_remote_copy(
                own_rows, out_rows.at[group], small_send.at[step - 1], small_recv.at[step - 1],
                device_id={"tp": lax.rem(group + step, groups)}, device_id_type=MESH,
            )
        )
    for step in range(1, shards):
        index = groups - 1 + step - 1
        small.append(
            pltpu.make_async_remote_copy(
                own_scales, out_scales.at[place], small_send.at[index], small_recv.at[index],
                device_id={"fs": lax.rem(place + step, shards)}, device_id_type=MESH,
            )
        )
    for copy in small:
        copy.start()

    copies = {}
    for number, (send, _) in enumerate(plan):
        array, chunk, pair, hop, kind = send
        step = hop if chunk % 2 == 0 else ring - hop
        owner = lax.rem(z + ring - step, ring) * 2 + (y if pair == 0 else 1 - y)
        slot = outs[array].at[owner, core, chunk]
        source = own[array].at[core, chunk] if (hop == 0 and pair == 0) else slot
        target = {"z": up if chunk % 2 == 0 else down, "y": across, "d": twin}[kind]
        copies[send] = pltpu.make_async_remote_copy(
            source, slot, send_sem.at[number], recv_sem.at[number],
            device_id=target, device_id_type=MESH,
        )

    local = [
        pltpu.make_async_copy(own[array], outs[array].at[place], local_sem.at[array])
        for array in range(count)
    ]
    local.append(pltpu.make_async_copy(own_rows, out_rows.at[group], local_sem.at[count]))
    local.append(pltpu.make_async_copy(own_scales, out_scales.at[place], local_sem.at[count + 1]))

    arrived = set()
    started_local = False
    for send, needs in plan:
        if needs is not None and needs not in arrived:
            if not started_local:
                started_local = True
                for copy in local:
                    copy.start()
            copies[needs].wait_recv()
            arrived.add(needs)
        copies[send].start()
    for send, _ in plan:
        copies[send].wait_send()
        if send not in arrived:
            copies[send].wait_recv()
    for copy in small:
        copy.wait()
    for copy in local:
        copy.wait()


def gather_all(arrays, rows, scales, groups, shards, reps):
    count = len(arrays)
    own = [a.reshape(reps, 4, a.shape[0] // (4 * reps), a.shape[1]) for a in arrays]
    sizes = [a.size // (4 * reps) * a.dtype.itemsize for a in arrays]
    plan = ring_plan(sizes, shards // 2)
    small = groups - 1 + shards - 1
    result = pl.pallas_call(
        functools.partial(gather_kernel, plan, count, groups, shards),
        out_shape=[jax.ShapeDtypeStruct((shards,) + a.shape, a.dtype) for a in own]
        + [
            jax.ShapeDtypeStruct((groups,) + rows.shape, rows.dtype),
            jax.ShapeDtypeStruct((shards,) + scales.shape, scales.dtype),
        ],
        in_specs=[pl.BlockSpec(memory_space=pl.ANY)] * (count + 2),
        out_specs=[pl.BlockSpec(memory_space=pl.ANY)] * (count + 2),
        scratch_shapes=[
            pltpu.SemaphoreType.DMA((len(plan),)),
            pltpu.SemaphoreType.DMA((len(plan),)),
            pltpu.SemaphoreType.DMA((count + 2,)),
            pltpu.SemaphoreType.DMA((small,)),
            pltpu.SemaphoreType.DMA((small,)),
        ],
        compiler_params=pltpu.CompilerParams(collective_id=0, has_side_effects=True),
        name="gather_all",
    )(*own, rows, scales)
    whole = [g.reshape((shards,) + a.shape) for g, a in zip(result, arrays)]
    return whole, result[count], result[count + 1]


def layer_kernel(
    channels, length,
    residual, mixer_gain, value_scale, input_scale, output_scale, taps, conv_gain, channel_gain,
    gate_scale, up_scale, out_scale, down_scale,
    *refs,
):
    raw, out_ref, refs = refs[:7], refs[7], refs[8:]
    bufs, refs = refs[:5], refs[5:]
    others, refs = refs[:7], refs[7:]
    stages, refs = refs[:7], refs[7:]
    (own_res, own_scales, res, scales, gains, mixes, after, normed, gate_buf, hidden, outgoing, from_x, to_z, from_z, to_x, whole_z, out_buf,
     raw_sem, z_send, z_recv, y_send, y_recv, t_send, t_recv, mx_send, mx_recv, mt_send, mt_recv,
     r_send, r_recv, s_send, s_recv, m_send, m_recv, px_send, px_recv, pz_send, pz_recv,
     zz_send, zz_recv, out_sem) = refs
    proj_buf, mout_buf, gate_w, up_w, down_w = bufs
    shards = gate_w.shape[0]
    place = lax.axis_index("fs")
    core = lax.axis_index("rep")
    group = lax.axis_index("tp")
    own_width, tokens = residual.shape
    mix_scales = (value_scale, input_scale, output_scale)
    features = 2 * own_width
    block = mout_buf.shape[-1]
    per_group = shards // 2
    depth = shards // 2
    width = gate_w.shape[-1]
    narrow = mixes.shape[-1]
    all_tokens = 2 * tokens

    z, y = place // 2, place % 2
    side = z % 2
    part_of = ((z + 1) // 2) % 2
    high = (z * 2 + y) // per_group
    pair = z + 1 - 2 * side
    inner = part_of == 1
    outer = part_of == 0
    opposite = 1 - z // 2
    levels = [z, pair, 1 + opposite, (depth - 1) * opposite]
    twin = {"rep": 1 - core}
    across = {"fs": z * 2 + 1 - y}
    beside = {"tp": 1 - group}
    mate = {"fs": pair * 2 + y}
    corner = {"fs": pair * 2 + y, "tp": 1 - group}

    def remote(source, target, send, recv, device):
        return pltpu.make_async_remote_copy(
            source, target, send, recv, device_id=device, device_id_type=MESH
        )

    def spot(array, owner, half):
        if array == 1:
            return mout_buf.at[owner, group, half]
        if array >= 2:
            return bufs[1 + array // 2].at[owner, half, array % 2]
        return proj_buf.at[owner, half]

    def owner_of(r, far):
        return levels[r] * 2 + (1 - y if far else y)

    def z_copy(array, way):
        target = spot(array, pair * 2 + y if way == 4 else place, core)
        if array == 1 or way in (2, 4):
            source = target
        else:
            source = others[array - 1 if array else 0]
        level = (None, pair, depth - 1 - z, depth - 1 - pair, depth - 1 - z)[way]
        kind = (None, 0, 2 - part_of, 2 - part_of, 2)[way]
        return remote(
            source, target, z_send.at[array, way - 1], z_recv.at[array, kind],
            {"fs": level * 2 + y},
        )

    def z_wait(array, r):
        target = spot(array, owner_of(r, False), core)
        remote(
            target, target, z_send.at[array, r - 1], z_recv.at[array, r - 1], across
        ).wait_recv()

    def y_copy(array, r):
        target = spot(array, owner_of(r, False), core)
        return remote(target, target, y_send.at[array, r], y_recv.at[array, r], across)

    def t_copy(array, r, far):
        target = spot(array, owner_of(r, far), core)
        index = r + 4 * far
        return remote(target, target, t_send.at[array, index], t_recv.at[array, index], twin)

    def mx_copy(r, far):
        target = spot(1, owner_of(r, far), core)
        index = r + 4 * far
        return remote(target, target, mx_send.at[index], mx_recv.at[index], beside)

    def mt_copy(r, far):
        target = mout_buf.at[owner_of(r, far), 1 - group, core]
        index = r + 4 * far
        return remote(target, target, mt_send.at[index], mt_recv.at[index], twin)

    rows = stages[0].shape[0]
    tall = stages[6].shape[1]
    raw_copies = []
    for i in range(4):
        raw_copies.append([pltpu.make_async_copy(
            raw[i].at[pl.ds(pl.multiple_of(core * rows, rows), rows)], stages[i], raw_sem.at[i])])
    for i in range(4, 6):
        raw_copies.append([pltpu.make_async_copy(
            raw[i].at[pl.ds(pl.multiple_of(core * rows, rows), rows)], stages[i], raw_sem.at[i])])
    raw_copies.append([
        pltpu.make_async_copy(
            raw[6].at[pl.ds(pl.multiple_of(k * width + core * tall, 16), tall)],
            stages[6].at[k], raw_sem.at[6 + k])
        for k in range(2)
    ])
    for group_of in raw_copies:
        for copy in group_of:
            copy.start()

    for first in range(0, own_width, tokens):
        own_res[:, first : first + tokens] = residual[first : first + tokens, :].T
    own_scales[...] = jnp.concatenate(
        [out_scale[...], down_scale[...], conv_gain[...], jnp.zeros((5, block), jnp.float32)], axis=0
    )

    barrier = pltpu.get_barrier_semaphore()
    partners = [{"fs": lax.rem(place + step, shards)} for step in range(1, shards)]
    partners += [beside, corner, twin]
    for other in partners:
        pl.semaphore_signal(barrier, inc=1, device_id=other, device_id_type=MESH)
    pl.semaphore_wait(barrier, len(partners))

    scale_copies = [
        remote(own_scales, scales.at[place], s_send.at[step], s_recv.at[step],
               {"fs": lax.rem(place + step, shards)})
        for step in range(1, shards)
    ]
    scale_copies.append(remote(own_scales, gains.at[group], s_send.at[0], s_recv.at[0], beside))
    res_z = remote(own_res, res.at[side, group], r_send.at[0], r_recv.at[0], mate)
    res_x = remote(own_res, res.at[side, group], r_send.at[1], r_recv.at[1], beside)
    passed = res.at[1 - side, group]
    res_d = remote(passed, passed, r_send.at[2], r_recv.at[2], beside)

    def start_z(*pairs):
        for array, r in pairs:
            z_copy(array, r).start()

    def start_inner(*pairs):
        @pl.when(inner)
        def _():
            for array, way in pairs:
                z_copy(array, way).start()

    def start_outer(*pairs):
        @pl.when(outer)
        def _():
            for array, way in pairs:
                z_copy(array, way).start()

    def wait_raw(*indices):
        for i in indices:
            for copy in raw_copies[i]:
                copy.wait()

    def both(first, second, size):
        return [
            (first, pl.ds(pl.multiple_of(part_of * size, 128), size)),
            (second, pl.ds(pl.multiple_of((1 - part_of) * size, 128), size)),
        ]

    res_z.start()
    res_x.start()
    wait_raw(0, 1, 2)
    for i in range(3):
        for target, cols in both(proj_buf.at[place, core], others[0], narrow):
            target[:, i * narrow : (i + 1) * narrow] = stages[i][:, cols].astype(jnp.bfloat16)
    start_z((0, 1), (0, 2), (0, 3))
    y_copy(0, 0).start()
    t_copy(0, 0, False).start()
    wait_raw(3)
    mout_buf[place, group, core] = stages[3][...].astype(jnp.bfloat16)
    start_z((1, 1), (1, 2), (1, 3))
    y_copy(1, 0).start()
    mx_copy(0, False).start()
    t_copy(1, 0, False).start()
    for copy in scale_copies:
        copy.start()
    fine = rows // 2
    for matrix in (1, 2):
        wait_raw(matrix + 3)
        for chunk in range(2):
            array = 2 * matrix + chunk
            lines = slice(chunk * fine, (chunk + 1) * fine)
            for target, cols in both(spot(array, place, core), others[array - 1], width):
                target[...] = stages[matrix + 3][lines, cols].astype(jnp.bfloat16)
            t_copy(array, 0, False).start()
            if matrix == 1:
                y_copy(array, 0).start()
                if chunk == 0:
                    start_z((array, 1))
                else:
                    start_outer((array, 1))
                start_inner((array, 2))
    wait_raw(6)
    short = tall // 2
    for chunk in range(2):
        array = 6 + chunk
        lines = slice(chunk * short, (chunk + 1) * short)
        down_w[place, core, chunk] = stages[6][part_of, lines, :].astype(jnp.bfloat16)
        others[array - 1][...] = stages[6][1 - part_of, lines, :].astype(jnp.bfloat16)
        t_copy(array, 0, False).start()
    res[side, group] = own_res[...]
    scales[place] = own_scales[...]
    gains[group] = own_scales[...]

    def take_z(array, r):
        z_wait(array, r)
        if r == 1 and array >= 2:
            start_inner((array, 4))
        y_copy(array, r).start()
        t_copy(array, r, False).start()
        if array == 1:
            mx_copy(r, False).start()

    def take_y(array, r):
        y_copy(array, r).wait_recv()
        t_copy(array, r, True).start()
        if array == 1:
            mx_copy(r, True).start()

    def run(items):
        for kind, array, r in items:
            if kind == "s":
                z_copy(array, r).start()
            elif kind == "o":
                y_copy(array, r).start()
            else:
                (take_z if kind == "z" else take_y)(array, r)

    def each(outer_items, inner_items):
        @pl.when(outer)
        def _():
            run(outer_items)

        @pl.when(inner)
        def _():
            run(inner_items)

    def finish(array):
        for far in (False, True):
            for r in range(4):
                t_copy(array, r, far).wait_recv()

    def scaled(squares, count):
        return lax.rsqrt(squares / count + epsilon)

    def normalize_side(s):
        floats = [res[s, k].astype(jnp.float32) for k in range(2)]
        squares = sum(jnp.sum(row * row, axis=1, keepdims=True) for row in floats)
        factor = scaled(squares, features)
        lines = pl.ds(pl.multiple_of(s * tokens, tokens), tokens)
        for k in range(2):
            cols = slice(k * own_width, (k + 1) * own_width)
            normed[lines, cols] = (
                res[s, k].astype(jnp.float32) * factor * mixer_gain[:, cols]
            ).astype(jnp.bfloat16)

    order = (1, 2, 3)
    take_z(0, 2)
    take_z(1, 2)
    for array in (4, 5):
        y_copy(array, 0).start()
    res_z.wait_recv()
    res_d.start()
    start_inner((2, 3), (3, 3))
    start_outer((2, 2), (3, 2))
    take_z(0, 1)
    take_z(0, 3)
    for array in (6, 7):
        y_copy(array, 0).start()
    res_x.wait_recv()
    normalize_side(side)
    for r in (0, 2, 1, 3):
        take_y(0, r)
    res_d.wait_recv()
    normalize_side(1 - side)
    finish(0)

    own_cols = pl.ds(pl.multiple_of(part_of * narrow, 128), narrow)

    def project(index):
        weight = proj_buf[:, :, :, index * narrow : (index + 1) * narrow].reshape(features, narrow)
        product = jnp.dot(normed[...], weight, preferred_element_type=jnp.float32)
        return product * mix_scales[index][:, own_cols]

    value = project(0)
    u = project(1) * value
    place_in = lax.rem(lax.broadcasted_iota(jnp.int32, u.shape, 0), length)
    one = jnp.where(place_in >= 1, pltpu.roll(u, 1, 0), 0.0)
    two = jnp.where(place_in >= 2, pltpu.roll(u, 2, 0), 0.0)
    conv = taps[2:3, own_cols] * u + taps[1:2, own_cols] * one + taps[0:1, own_cols] * two
    mixes[group, part_of] = (project(2) * conv).astype(jnp.bfloat16)
    mix_slot = mixes.at[group, part_of]
    mix_copies = [
        remote(mix_slot, mix_slot, m_send.at[i], m_recv.at[i], device)
        for i, device in enumerate((mate, beside, corner))
    ]
    for copy in mix_copies:
        copy.start()
    start_inner((3, 1))
    start_z((4, 1), (5, 1))
    start_outer((4, 2), (5, 2))
    start_z((6, 1), (7, 1))
    each(
        [("z", 1, 3), ("z", 2, 2), ("z", 2, 3), ("z", 1, 1), ("z", 3, 2), ("z", 3, 3)],
        [("z", 1, 1), ("z", 1, 3), ("z", 2, 2), ("z", 3, 2), ("z", 2, 1), ("z", 3, 1),
         ("s", 4, 2), ("s", 4, 3), ("s", 5, 2), ("s", 5, 3)],
    )
    for r in (0, 2, 1, 3):
        take_y(1, r)
    for far in (False, True):
        for r in range(4):
            mx_copy(r, far).wait_recv()
            mt_copy(r, far).start()
    each([("z", 2, 1)], [])
    for copy in scale_copies + mix_copies:
        copy.wait_recv()
    finish(1)
    for far in (False, True):
        for r in range(4):
            mt_copy(r, far).wait_recv()
    total = jnp.zeros((all_tokens, 1), jnp.float32)
    for k in range(2):
        for b in range(2):
            lines = mixes[k, b].astype(jnp.float32)
            total = total + jnp.sum(lines * lines, axis=1, keepdims=True)
    factor = scaled(total, channels)
    for k in range(2):
        for b in range(2):
            cols = slice((2 * k + b) * narrow, (2 * k + b + 1) * narrow)
            hidden[:, cols] = (
                mixes[k, b].astype(jnp.float32) * factor
                * gains[k, 2:3, b * narrow : (b + 1) * narrow]
            ).astype(jnp.bfloat16)
    squares = jnp.zeros((all_tokens, 1), jnp.float32)
    for s in range(shards):
        k, inside = s // per_group, (s % per_group) * block
        part = jnp.dot(
            hidden[:, : 4 * narrow], mout_buf[s].reshape(4 * narrow, block),
            preferred_element_type=jnp.float32,
        ) * scales[s, 0:1, :]
        base = res[:, k, :, inside : inside + block].reshape(all_tokens, block)
        row = (base.astype(jnp.float32) + part).astype(jnp.bfloat16)
        after[s] = row
        row = row.astype(jnp.float32)
        squares = squares + jnp.sum(row * row, axis=1, keepdims=True)
    factor = scaled(squares, features)
    for s in range(shards):
        cols = slice(s * block, (s + 1) * block)
        normed[:, cols] = (
            after[s].astype(jnp.float32) * factor * channel_gain[:, cols]
        ).astype(jnp.bfloat16)

    def tiles(body):
        tile = 256
        whole = width // tile

        @pl.loop(0, whole)
        def _(j):
            body(pl.multiple_of(j * tile, tile), tile)

        if width % tile:
            body(whole * tile, width % tile)

    def multiply(weights, start, size):
        weight = weights[:, :, :, :, pl.ds(start, size)].reshape(features, size)
        return jnp.dot(normed[...], weight, preferred_element_type=jnp.float32)

    def scale_at(scale, start, size):
        first = part_of * (width // 128) + start // 128
        lines = [scale[pl.ds(first + i, 1), :] for i in range(size // 128)]
        return jnp.concatenate(lines, axis=1)

    def gate_tile(start, size):
        gate_buf[:, pl.ds(start, size)] = multiply(gate_w, start, size) * scale_at(
            gate_scale, start, size
        )

    def up_tile(start, size):
        product = multiply(up_w, start, size) * scale_at(up_scale, start, size)
        gate = gate_buf[:, pl.ds(start, size)]
        hidden[:, pl.ds(start, size)] = (
            gate / (1.0 + jnp.exp(-gate)) * product
        ).astype(jnp.bfloat16)

    each(
        [("z", 4, 2), ("z", 4, 3), ("z", 3, 1), ("z", 5, 2), ("z", 5, 3)],
        [("z", 2, 3), ("z", 3, 3), ("z", 4, 1), ("z", 5, 1), ("s", 6, 2), ("s", 7, 2)],
    )
    for array in (2, 3):
        for r in (0,) + order:
            take_y(array, r)
    finish(2)
    finish(3)
    tiles(gate_tile)
    each(
        [("s", 6, 2), ("s", 7, 2),
         ("z", 4, 1), ("z", 5, 1), ("z", 6, 1), ("z", 7, 1),
         ("y", 4, 0), ("y", 5, 0), ("y", 4, 2), ("y", 4, 3), ("y", 5, 2), ("y", 5, 3),
         ("y", 4, 1), ("y", 5, 1)],
        [("z", 4, 2), ("z", 5, 2), ("z", 4, 3), ("z", 5, 3), ("s", 6, 3), ("s", 7, 3),
         ("z", 6, 1), ("z", 7, 1), ("y", 4, 0), ("y", 5, 0), ("y", 4, 1), ("y", 5, 1),
         ("y", 4, 2), ("y", 5, 2), ("z", 6, 2), ("z", 7, 2), ("y", 4, 3), ("y", 5, 3)],
    )
    finish(4)
    finish(5)
    tiles(up_tile)

    steps = [(r, far) for r in range(4) for far in (False, True)]

    def index_of(k):
        return owner_of(*steps[k])

    def mine(k):
        return (high == group) if k < per_group else (high != group)

    def slot_of(k):
        return lax.rem(index_of(k), per_group)

    last = shards - 1
    strip = tokens // 2

    def px_copy(k, which):
        sems = px_send.at[k, which], px_recv.at[k, which], beside
        if k == last:
            lines = pl.ds(which * strip, strip)
            return remote(to_x.at[k, lines], from_x.at[k, side, lines], *sems)
        who = 1 - side if which == 0 else side
        source = to_x.at[k] if k % 2 else outgoing.at[k, who]
        return remote(source, from_x.at[k, who], *sems)

    def pz_copy(k):
        i = slot_of(k)
        return remote(to_z.at[i], from_z.at[i], pz_send.at[i], pz_recv.at[i], mate)

    def zz_copies(k):
        s = index_of(k)
        mates = outgoing.at[k, 1 - side]
        if k < last:
            return [remote(mates, whole_z.at[s], zz_send.at[s], zz_recv.at[s], mate)]
        copies = []
        for half, index in ((0, s), (1, shards)):
            lines = pl.ds(half * strip, strip)
            copies.append(remote(
                outgoing.at[k, 1 - side, lines], whole_z.at[s, lines],
                zz_send.at[index], zz_recv.at[index], mate,
            ))
        return copies

    def down(k):
        r, far = steps[k]
        for array in (6, 7):
            t_copy(array, r, far).wait_recv()
        s = index_of(k)
        weight = down_w[s].reshape(width, block)
        part = jnp.dot(hidden[...], weight, preferred_element_type=jnp.float32)
        part = (part * scales[s, 1:2, :]).astype(jnp.bfloat16)
        outgoing[k, 0] = part[:tokens]
        outgoing[k, 1] = part[tokens:]

        if k % 2:
            for copy in zz_copies(k):
                copy.start()
            return

        @pl.when(jnp.logical_not(mine(k)))
        def _():
            px_copy(k, 0).start()
            if k % per_group:
                px_copy(k - 2, 1).start()
                px_copy(k, 1).start()

    def pass_on(k):
        if k % 2:
            copies = zz_copies(k)
            for which, copy in enumerate(copies):
                copy.wait_recv()
                size = tokens // len(copies)
                lines = slice(which * size, (which + 1) * size)

                @pl.when(jnp.logical_not(mine(k)))
                def _():
                    to_x[k, lines] = (
                        outgoing[k, side, lines].astype(jnp.float32)
                        + whole_z[index_of(k), lines].astype(jnp.float32)
                    ).astype(jnp.bfloat16)
                    px_copy(k, which if k == last else 1).start()

            return

        @pl.when(mine(k))
        def _():
            px_copy(k, 0).wait_recv()
            to_z[slot_of(k)] = (
                outgoing[k, 1 - side].astype(jnp.float32) + from_x[k, 1 - side].astype(jnp.float32)
            ).astype(jnp.bfloat16)
            pz_copy(k).start()

    def out_copy(k):
        i = slot_of(k)
        target = out_ref.at[:, pl.ds(pl.multiple_of(i * block, block), block)]
        return pltpu.make_async_copy(out_buf.at[i], target, out_sem.at[i])

    def close(k):
        i = slot_of(k)
        s = index_of(k)

        @pl.when(mine(k))
        def _():
            px_copy(k, 1).wait_recv()
            if k == last:
                px_copy(k, 0).wait_recv()
            if k % 2 == 0:
                pz_copy(k).wait_recv()
            lines = pl.ds(pl.multiple_of(side * tokens, tokens), tokens)
            total = outgoing[k, side].astype(jnp.float32) + from_x[k, side].astype(jnp.float32)
            total = total + (whole_z[s] if k % 2 else from_z[i]).astype(jnp.float32)
            out_buf[i] = (after[s, lines, :].astype(jnp.float32) + total).astype(jnp.bfloat16)
            out_copy(k).start()

    def take_all(take, r):
        for array in (6, 7):
            take(array, r)

    def early_waits():
        z_copy(0, 3).wait_send()
        z_copy(1, 3).wait_send()

        @pl.when(inner)
        def _():
            for array in range(2, 8):
                for way in (3, 4):
                    z_copy(array, way).wait_send()

        for array in range(8):
            for r in range(4):
                if r in (1, 2):
                    z_copy(array, r).wait_send()
                if array < 6 or r < 3:
                    y_copy(array, r).wait_send()
                    for far in (False, True):
                        t_copy(array, r, far).wait_send()
        for r in range(4):
            for far in (False, True):
                mx_copy(r, far).wait_send()
                mt_copy(r, far).wait_send()
        for copy in scale_copies + mix_copies + [res_z, res_x, res_d]:
            copy.wait_send()

    each([("z", 6, 2), ("z", 7, 2)], [])
    down(0)
    take_all(take_y, 0)
    down(1)
    down(2)
    take_all(take_y, 1)
    each([("z", 6, 3), ("z", 7, 3)], [])
    down(3)
    down(4)
    each([], [("z", 6, 3), ("z", 7, 3)])
    take_all(take_y, 2)
    down(5)
    down(6)
    pass_on(1)
    pass_on(3)
    pass_on(0)
    pass_on(4)
    early_waits()
    take_y(6, 3)
    pass_on(2)
    take_y(7, 3)
    down(7)
    pass_on(5)
    pass_on(6)
    close(0)
    close(2)
    close(4)
    pass_on(7)
    for k in (1, 3, 6, 5, 7):
        close(k)

    for array in (6, 7):
        y_copy(array, 3).wait_send()
        t_copy(array, 3, False).wait_send()
        t_copy(array, 3, True).wait_send()
    for k in range(shards):
        if k % 2:
            for copy in zz_copies(k):
                copy.wait_send()
        else:
            pl.when(mine(k))(pz_copy(k).wait_send)

        @pl.when(jnp.logical_not(mine(k)))
        def _():
            if k % 2 == 0 or k == last:
                px_copy(k, 0).wait_send()
            px_copy(k, 1).wait_send()

    for k in range(shards):
        pl.when(mine(k))(out_copy(k).wait)


def fused(
    shards, residual, small, raw,
):
    own_width, tokens = residual.shape
    features = 2 * own_width
    short = jnp.bfloat16
    in_rows, mix_width = raw[0].shape
    rows, narrow = in_rows // 2, mix_width // 2
    ff = raw[4].shape[1]
    width = ff // 2
    out_rows, block = raw[3].shape
    channels = 2 * out_rows
    tall = width // 2
    steps = shards
    vmem = pl.BlockSpec(memory_space=pltpu.VMEM)
    dma = pltpu.SemaphoreType.DMA
    return pl.pallas_call(
        functools.partial(layer_kernel, channels, LEN),
        out_shape=jax.ShapeDtypeStruct((tokens, own_width), short),
        in_specs=[vmem] * (1 + len(small)) + [pl.BlockSpec(memory_space=pl.ANY)] * 7,
        out_specs=pl.BlockSpec(memory_space=pl.ANY),
        scratch_shapes=[
            pltpu.VMEM((shards, 2, rows, 3 * narrow), short),
            pltpu.VMEM((shards, 2, 2, out_rows // 2, block), short),
            pltpu.VMEM((shards, 2, 2, rows // 2, width), short),
            pltpu.VMEM((shards, 2, 2, rows // 2, width), short),
            pltpu.VMEM((shards, 2, 2, tall // 2, block), short),
            pltpu.VMEM((rows, 3 * narrow), short),
            pltpu.VMEM((rows // 2, width), short),
            pltpu.VMEM((rows // 2, width), short),
            pltpu.VMEM((rows // 2, width), short),
            pltpu.VMEM((rows // 2, width), short),
            pltpu.VMEM((tall // 2, block), short),
            pltpu.VMEM((tall // 2, block), short),
        ]
        + [pltpu.VMEM((rows, mix_width), jnp.float32)] * 3
        + [
            pltpu.VMEM((out_rows // 2, block), jnp.float32),
            pltpu.VMEM((rows, ff), jnp.float32),
            pltpu.VMEM((rows, ff), jnp.float32),
            pltpu.VMEM((2, tall, block), jnp.float32),
            pltpu.VMEM((tokens, own_width), short),
            pltpu.VMEM((8, block), jnp.float32),
            pltpu.VMEM((2, 2, tokens, own_width), short),
            pltpu.VMEM((shards, 8, block), jnp.float32),
            pltpu.VMEM((2, 8, block), jnp.float32),
            pltpu.VMEM((2, 2, 2 * tokens, narrow), short),
            pltpu.VMEM((shards, 2 * tokens, block), short),
            pltpu.VMEM((2 * tokens, features), short),
            pltpu.VMEM((2 * tokens, width), jnp.float32),
            pltpu.VMEM((2 * tokens, width), short),
            pltpu.VMEM((steps, 2, tokens, block), short),
            pltpu.VMEM((steps, 2, tokens, block), short),
            pltpu.VMEM((steps // 2, tokens, block), short),
            pltpu.VMEM((steps // 2, tokens, block), short),
            pltpu.VMEM((steps, tokens, block), short),
            pltpu.VMEM((steps, tokens, block), short),
            pltpu.VMEM((steps // 2, tokens, block), short),
            dma((8,)),
            dma((8, 4)),
            dma((8, 3)),
            dma((8, 4)),
            dma((8, 4)),
            dma((8, 8)),
            dma((8, 8)),
            dma((8,)),
            dma((8,)),
            dma((8,)),
            dma((8,)),
            dma((3,)),
            dma((3,)),
            dma((shards,)),
            dma((shards,)),
            dma((3,)),
            dma((3,)),
            dma((steps, 2)),
            dma((steps, 2)),
            dma((steps // 2,)),
            dma((steps // 2,)),
            dma((steps + 1,)),
            dma((steps + 1,)),
            dma((steps // 2,)),
        ],
        compiler_params=pltpu.CompilerParams(
            collective_id=1, has_side_effects=True, vmem_limit_bytes=60 * 1024 * 1024
        ),
        name="layer",
    )(
        residual, *small, *raw,
    )


def local(
    reps,
    shards,
    groups,
    residual,
    mixer_gain,
    value_weight,
    value_scale,
    input_gate_weight,
    input_gate_scale,
    output_gate_weight,
    output_gate_scale,
    conv_taps,
    conv_gain,
    mixer_out_weight,
    mixer_out_scale,
    channel_gain,
    gate_weight,
    gate_scale,
    up_weight,
    up_scale,
    down_weight,
    down_scale,
):
    own_rows, tokens = residual.shape
    width = value_weight.shape[1]
    channels = width * groups
    features = own_rows * groups
    short = jnp.bfloat16
    block, ff = mixer_out_weight.shape[1], gate_weight.shape[1]
    in_rows, out_rows = value_weight.shape[0], mixer_out_weight.shape[0]
    if (
        reps == 2 and groups == 2 and shards == 8 and tokens % LEN == 0
        and block % 128 == 0 and width % 256 == 0 and ff % 256 == 0 and block == width
        and in_rows % 64 == 0 and out_rows == width and own_rows == block * shards // 2
    ):
        result = fused(
            shards, residual,
            [mixer_gain[None], value_scale[None], input_gate_scale[None], output_gate_scale[None],
             conv_taps, conv_gain[None], channel_gain[None], gate_scale.reshape(-1, 128),
             up_scale.reshape(-1, 128), mixer_out_scale[None], down_scale[None]],
            [value_weight, input_gate_weight, output_gate_weight, mixer_out_weight,
             gate_weight, up_weight, down_weight],
        )
        return result.T
    projections = jnp.concatenate(
        [value_weight.astype(short), input_gate_weight.astype(short), output_gate_weight.astype(short)],
        axis=1,
    )
    arrays = [
        projections,
        mixer_out_weight.astype(short),
        gate_weight.astype(short),
        up_weight.astype(short),
        down_weight.astype(short),
    ]
    scales = jnp.stack([mixer_out_scale, down_scale])
    (proj_all, out_all, gate_all, up_all, down_all), rows_all, scales_all = gather_all(
        arrays, residual, scales, groups, shards, reps
    )
    whole = rows_all.reshape(features, tokens)
    out_scale = scales_all[:, 0].reshape(features)
    down_scale_full = scales_all[:, 1].reshape(features)

    normed = normalize(whole, mixer_gain)
    projected = contract(proj_all.reshape(features, 3 * width), normed)
    value = projected[:width] * value_scale[:, None]
    in_gate = projected[width : 2 * width] * input_gate_scale[:, None]
    out_gate = projected[2 * width :] * output_gate_scale[:, None]
    mixed = out_gate * causal_conv(in_gate * value, conv_taps, LEN)
    squares = lax.psum(jnp.sum(mixed * mixed, axis=0), "tp")
    conv_normed = (
        mixed * lax.rsqrt(squares / channels + epsilon)[None, :] * conv_gain[:, None]
    ).astype(short)
    part = lax.dot_general(
        out_all, conv_normed, (((1,), (0,)), ((), ())), preferred_element_type=jnp.float32
    ).reshape(features, tokens)
    rounded = (part * out_scale[:, None]).astype(short)
    parts = lax.all_gather(rounded, "tp", axis=0)
    total = jnp.sum(parts.astype(jnp.float32), axis=0)
    after_whole = (whole.astype(jnp.float32) + total).astype(short)
    after_own = lax.dynamic_slice_in_dim(
        after_whole, lax.axis_index("tp") * own_rows, own_rows, 0
    )
    normed_two = normalize(after_whole, channel_gain)
    gate = contract(gate_all.reshape(features, -1), normed_two)
    upper = contract(up_all.reshape(features, -1), normed_two)
    hidden = (jax.nn.silu(gate * gate_scale[:, None]) * (upper * up_scale[:, None])).astype(short)
    down = lax.dot_general(
        down_all, hidden, (((1,), (0,)), ((), ())), preferred_element_type=jnp.float32
    ).reshape(features, tokens)
    total_two = lax.psum_scatter(
        (down * down_scale_full[:, None]).astype(short),
        "tp",
        scatter_dimension=0,
        tiled=True,
    ).astype(jnp.float32)
    return (after_own.astype(jnp.float32) + total_two).astype(short)


def solution(mesh):
    placed = (
        P("tp", ("rep", "fs")),
        P(),
        P("fs", "tp"),
        P("tp"),
        P("fs", "tp"),
        P("tp"),
        P("fs", "tp"),
        P("tp"),
        P(None, "tp"),
        P("tp"),
        P("tp", "fs"),
        P("fs"),
        P(),
        P("fs", "tp"),
        P("tp"),
        P("fs", "tp"),
        P("tp"),
        P("tp", "fs"),
        P("fs"),
    )
    sizes = mesh.shape["rep"], mesh.shape["fs"], mesh.shape["tp"]
    return jax.shard_map(
        functools.partial(local, *sizes),
        mesh=mesh,
        in_specs=placed,
        out_specs=P("tp", ("rep", "fs")),
        check_vma=False,
    )
```
